256 devices in a mesh: grp: 2 (over y), sp: 16 (over z), fs: 4 (over x), tp: 2 (over core).
Axes of the slice: x: 4, y: 2, z: 16, core: 2. Of those that a mesh axis runs over, the one named last changes fastest.
The devices are a block of a 4x16x16 slice.
Arguments:
- tokens: bfloat16 [8, 4096, 2048], P(('grp', 'fs'), 'sp', 'tp'), parts along dimension 0, may hold values from -6 to 6
- input_norm_gain: float32 [2048], replicated, may hold values from 0.1 to 1.9
- query_weight: bfloat16 [2048, 1024], P('sp', 'tp'), may hold values from -0.125 to 0.125
- key_weight: bfloat16 [2048, 1024], P('sp', 'tp'), may hold values from -0.125 to 0.125
- value_weight: bfloat16 [2048, 1024], P('sp', 'tp'), may hold values from -0.125 to 0.125
- decay_gate_weight: bfloat16 [2048, 8], replicated, may hold values from -0.125 to 0.125
- write_strength_weight: bfloat16 [2048, 8], replicated, may hold values from -0.125 to 0.125
- up_weight: bfloat16 [2048, 1024], P('sp', 'tp'), may hold values from -0.125 to 0.125
- gate_half_weight: bfloat16 [2048, 1024], P('sp', 'tp'), may hold values from -0.125 to 0.125
- log_decay_rate: float32 [8], replicated, may hold values from -30 to 0
- write_strength_bias: float32 [8], replicated, may hold values from -7 to 1
- decay_spike_added: float32 [8, 4096, 8], P(('grp', 'fs'), 'sp', 'tp'), parts along dimension 0, may hold values from -2 to 0
- starting_state: float32 [8, 8, 128, 128], P(('grp', 'fs'), 'tp'), parts along dimension 0, may hold values from -4 to 4
- head_norm_gain: float32 [128], replicated, may hold values from 0.1 to 1.9
- convolution_kernel: float32 [31, 1024], replicated, may hold values from -4 to 4
- channel_norm_gain: float32 [1024], replicated, may hold values from 0.1 to 1.9
- delta_output_rows: bfloat16 [1024, 2048], P('tp', 'sp'), may hold values from -0.125 to 0.125
- convolution_output_rows: bfloat16 [1024, 2048], P('tp', 'sp'), may hold values from -0.125 to 0.125
Outputs:
- mixed: bfloat16 [8, 4096, 2048], P(('grp', 'fs'), 'sp', 'tp'), parts along dimension 0
The draws below stay inside these ranges and needn't reach their ends.
There are 2 independent parts, one for each index of `grp`. The reference program is written for one: setup_inputs(seed, part) draws one part's arguments, and reference() takes and returns one part's arrays. A program takes and returns all parts, laid end to end along the dimension named above; an argument that names none is the same for every part. Nothing has to cross between parts.
All inputs are finite; a program needn't handle non-finite values.
Results may differ from the reference program's by a relative error of at most 0.01.
Values may be sent and summed in bfloat16 or wider, within the bound.
A program may use at most 64 MiB of HBM per device.

```python
import math
import jax
import jax.numpy as jnp
from jax import lax

D = 2048
HEADS = 8
HEAD = 128
CH = 1024
KSIZE = 31
BLOCK = 64
TOK_DEV = 256
LEN = 4096
SEQS = 4
WIDTH_A = 1024
N_TP = 2


def fast_heads(key, fast_count):
    order = jax.random.permutation(jax.random.fold_in(key, 11), HEADS)
    return order < fast_count


def draw_log_decay_rate(key, part):
    fast_key = jax.random.fold_in(key, 12)
    slow_key = jax.random.fold_in(key, 13)
    fast_count = HEADS // 2
    fast_mask = fast_heads(key, fast_count)
    fast_rate = jnp.exp(jax.random.uniform(fast_key, (HEADS,), jnp.float32, math.log(1.0 / 60.0), math.log(1.0 / 30.0))) / 0.7
    slow_rate = 0.5 / (0.7 * LEN) * jnp.exp(jax.random.uniform(slow_key, (HEADS,), jnp.float32, math.log(0.5), 0.0))
    return jnp.log(jnp.where(fast_mask, fast_rate, slow_rate)).astype(jnp.float32)


def draw_write_strength_bias(key, part):
    fast_key = jax.random.fold_in(key, 31)
    slow_key = jax.random.fold_in(key, 32)
    fast_count = HEADS // 2
    fast_mask = fast_heads(key, fast_count)
    fast_level = jax.random.uniform(fast_key, (HEADS,), jnp.float32, -1.0, 1.0)
    slow_level = math.log(0.5 * HEAD / LEN) + jax.random.uniform(slow_key, (HEADS,), jnp.float32, math.log(0.5), 0.0)
    return jnp.where(fast_mask, fast_level, slow_level).astype(jnp.float32)


def draw_decay_spike_added(key, part):
    level_key = jax.random.fold_in(key, 21)
    place_key = jax.random.fold_in(key, 22)
    depth_key = jax.random.fold_in(key, 23)
    blocks = LEN // TOK_DEV
    decay_levels = jax.random.uniform(level_key, (SEQS, blocks, HEADS), jnp.float32, 0.0, 1.0) * (-1.0 / LEN)
    decay_levels = jnp.repeat(decay_levels, TOK_DEV, axis=1)
    places = jax.random.randint(place_key, (SEQS, 2, HEADS), 0, LEN)
    sequence_depths = jnp.log(jax.random.uniform(depth_key, (SEQS, 2, HEADS), jnp.float32, 0.6, 0.8))
    positions = jnp.arange(LEN, dtype=jnp.int32)
    spike_applied = positions[None, :, None, None] == places[:, None, :, :]
    decay_spikes = jnp.sum(jnp.where(spike_applied, sequence_depths[:, None, :, :], 0.0), axis=2)
    return (decay_levels + decay_spikes).astype(jnp.float32)


def draw_convolution_kernel(key, part):
    raw = jnp.clip(jax.random.normal(key, (KSIZE, CH), jnp.float32), -6.0, 6.0)
    channel = jnp.arange(CH, dtype=jnp.float32) / CH
    scales = jnp.exp(math.log(10.0) * channel - 0.5 * math.log(10.0))
    return (raw * KSIZE ** (-0.5) * scales[None, :]).astype(jnp.float32)


def steps_of(stream_key, extent, split, least, largest):
    gain = 1.0
    for dim, shards_of in split:
        steps = jax.random.uniform(jax.random.fold_in(jax.random.fold_in(stream_key, 6), dim), (shards_of,), jnp.float32, least / len(split), largest / len(split))
        gain = gain * jnp.repeat(jnp.exp(steps), extent[dim] // shards_of).reshape((-1,) + (1,) * (len(extent) - 1 - dim))
    return gain


def bell_draw(own_key, dims, width, most, pieces=(), kind=jnp.bfloat16):
    result = width * jax.random.normal(own_key, dims, jnp.float32)
    if pieces:
        result = result * steps_of(own_key, dims, pieces, -0.22, 0.18)
    return jnp.clip(result, -most, most).astype(kind)


def setup_inputs(seed: int = 0, part: int = 0) -> dict:
    splits = jax.random.split(jax.random.key(seed), 19)
    part_keys = jax.random.split(jax.random.fold_in(splits[18], part), 19)
    tokens = bell_draw(part_keys[0], (SEQS, LEN, D), 1.0, 6.0, ((0, 4), (1, 16), (2, 2)))
    input_norm_gain = jnp.clip(1.0 + 0.18 * jax.random.normal(splits[1], (D,), jnp.float32), 0.1, 1.9)
    query_weight = bell_draw(splits[2], (D, WIDTH_A), D ** -0.5, 0.125, ((0, 16), (1, 2)))
    key_weight = bell_draw(splits[3], (D, WIDTH_A), D ** -0.5, 0.125, ((0, 16), (1, 2)))
    value_weight = bell_draw(splits[4], (D, WIDTH_A), D ** -0.5, 0.125, ((0, 16), (1, 2)))
    decay_gate_weight = bell_draw(splits[5], (D, HEADS), D ** -0.5, 0.125)
    write_strength_weight = bell_draw(splits[6], (D, HEADS), D ** -0.5, 0.125)
    up_weight = bell_draw(splits[7], (D, CH), D ** -0.5, 0.125, ((0, 16), (1, 2)))
    gate_half_weight = bell_draw(splits[8], (D, CH), D ** -0.5, 0.125, ((0, 16), (1, 2)))
    log_decay_rate = draw_log_decay_rate(jax.random.fold_in(splits[18], 71), part)
    write_strength_bias = draw_write_strength_bias(jax.random.fold_in(splits[18], 71), part)
    decay_spike_added = draw_decay_spike_added(jax.random.fold_in(jax.random.fold_in(splits[18], part), 71), part)
    starting_state = bell_draw(part_keys[12], (SEQS, HEADS, HEAD, HEAD), 0.5, 4.0, ((0, 4), (1, 2)), jnp.float32)
    head_norm_gain = jnp.clip(1.0 + 0.18 * jax.random.normal(splits[13], (HEAD,), jnp.float32), 0.1, 1.9)
    convolution_kernel = draw_convolution_kernel(jax.random.fold_in(splits[18], 71), part)
    channel_norm_gain = jnp.clip(1.0 + 0.18 * jax.random.normal(splits[15], (CH,), jnp.float32), 0.1, 1.9)
    delta_output_rows = bell_draw(splits[16], (WIDTH_A, D), (WIDTH_A + CH) ** -0.5, 0.125, ((0, 2), (1, 16)))
    convolution_output_rows = bell_draw(splits[17], (CH, D), (WIDTH_A + CH) ** -0.5, 0.125, ((0, 2), (1, 16)))
    return dict(tokens=tokens, input_norm_gain=input_norm_gain, query_weight=query_weight, key_weight=key_weight, value_weight=value_weight, decay_gate_weight=decay_gate_weight, write_strength_weight=write_strength_weight, up_weight=up_weight, gate_half_weight=gate_half_weight, log_decay_rate=log_decay_rate, write_strength_bias=write_strength_bias, decay_spike_added=decay_spike_added, starting_state=starting_state, head_norm_gain=head_norm_gain, convolution_kernel=convolution_kernel, channel_norm_gain=channel_norm_gain, delta_output_rows=delta_output_rows, convolution_output_rows=convolution_output_rows)


EPS = 1e-06
HIGH = lax.Precision.HIGHEST

def unit_rows(values):
    return values * lax.rsqrt(lax.optimization_barrier(jnp.sum(values * values, axis=-1, keepdims=True)) + EPS)

def rounded(values):
    return lax.optimization_barrier(values.astype(jnp.bfloat16)).astype(jnp.float32)

def block_terms(query, keys, values, log_decay, beta):
    rows = keys.shape[0]
    count = rows // BLOCK

    def split_blocks(array):
        return jnp.swapaxes(array.reshape((count, BLOCK) + array.shape[1:]), 1, 2)
    q_blocks, k_blocks, v_blocks = (split_blocks(query), split_blocks(keys), split_blocks(values))
    g_blocks, b_blocks = (split_blocks(log_decay), split_blocks(beta))
    cumdec = jnp.cumsum(g_blocks, axis=-1)
    lower = jnp.tril(jnp.ones((BLOCK, BLOCK), bool))
    strict = jnp.tril(jnp.ones((BLOCK, BLOCK), bool), -1)
    diff = cumdec[..., :, None] - cumdec[..., None, :]
    gamma = jnp.where(lower, jnp.exp(jnp.where(lower, diff, 0.0)), 0.0)
    k_beta = k_blocks * b_blocks[..., None]
    a_matrix = jnp.where(strict, jnp.einsum('nhid,nhjd->nhij', k_beta, k_blocks, precision=HIGH) * gamma, 0.0)
    left_side = a_matrix + jnp.eye(BLOCK, dtype=jnp.float32)
    right_side = jnp.concatenate([v_blocks * b_blocks[..., None], k_beta * jnp.exp(cumdec)[..., None]], axis=-1)
    solved = jax.scipy.linalg.solve_triangular(left_side, right_side, lower=True, unit_diagonal=True)
    width_v = v_blocks.shape[-1]
    updates, w_rows = (solved[..., :width_v], solved[..., width_v:])
    q_k = jnp.where(lower, jnp.einsum('nhid,nhjd->nhij', q_blocks, k_blocks, precision=HIGH) * gamma, 0.0)
    last = cumdec[..., -1]
    k_decayed = k_blocks * jnp.exp(last[..., None] - cumdec)[..., None]
    q_decayed = q_blocks * jnp.exp(cumdec)[..., None]
    return (q_decayed, k_decayed, updates, w_rows, q_k, last)

def block_outputs(start_state, terms):

    def advance(state, input_rows):
        q_decayed, k_decayed, updates, w_rows, q_k, last = input_rows
        v_new = updates - jnp.einsum('hcd,hde->hce', w_rows, state, precision=HIGH)
        output = jnp.einsum('hcd,hde->hce', q_decayed, state, precision=HIGH) + jnp.einsum('hij,hje->hie', q_k, v_new, precision=HIGH)
        state = state * jnp.exp(last)[..., None, None] + jnp.einsum('hcd,hce->hde', k_decayed, v_new, precision=HIGH)
        return (state, output)
    _, outputs = lax.scan(advance, start_state, terms)
    count, heads, blen, width_v = outputs.shape
    return jnp.swapaxes(outputs, 1, 2).reshape(count * blen, heads, width_v)

def single_sequence(tokens, decay_spike_added, starting_state, input_norm_gain, query_weight, key_weight, value_weight, decay_gate_weight, write_strength_weight, up_weight, gate_half_weight, log_decay_rate, write_strength_bias, head_norm_gain, convolution_kernel, channel_norm_gain, delta_output_rows, convolution_output_rows):
    rows = tokens.shape[0]
    token_f = tokens.astype(jnp.float32)
    normed = (token_f * lax.rsqrt(lax.optimization_barrier(jnp.mean(token_f * token_f, axis=-1, keepdims=True)) + EPS) * input_norm_gain).astype(jnp.bfloat16)

    def project_input(weight):
        return rounded(jnp.dot(normed.astype(jnp.float32), weight.astype(jnp.float32), preferred_element_type=jnp.float32))
    shape = (rows, HEADS, HEAD)
    query = unit_rows(jax.nn.silu(project_input(query_weight)).reshape(shape)) * HEAD ** (-0.5)
    keys = unit_rows(jax.nn.silu(project_input(key_weight)).reshape(shape))
    values = jax.nn.silu(project_input(value_weight)).reshape(shape)
    log_decay = -jnp.exp(log_decay_rate) * jax.nn.softplus(project_input(decay_gate_weight)) + decay_spike_added
    beta = jax.nn.sigmoid(project_input(write_strength_weight) + write_strength_bias)
    terms = block_terms(query, keys, values, log_decay, beta)
    attn = block_outputs(starting_state, terms)
    attn_out = (attn * lax.rsqrt(lax.optimization_barrier(jnp.mean(attn * attn, axis=-1, keepdims=True)) + EPS) * head_norm_gain).astype(jnp.bfloat16)
    attn_out = attn_out.reshape(rows, HEADS * HEAD)
    glu = lax.optimization_barrier((project_input(up_weight) * jax.nn.sigmoid(project_input(gate_half_weight))).astype(jnp.bfloat16))
    padded = jnp.concatenate([jnp.zeros((KSIZE - 1, CH), jnp.float32), glu.astype(jnp.float32)], axis=0)
    conv = jnp.zeros((rows, CH), jnp.float32)
    for tap in range(KSIZE):
        conv = conv + convolution_kernel[tap] * padded[tap:tap + rows]
    mean_c = lax.optimization_barrier(jnp.mean(conv, axis=-1, keepdims=True))
    var_c = lax.optimization_barrier(jnp.mean(conv * conv, axis=-1, keepdims=True)) - mean_c * mean_c
    conv_out = jax.nn.silu((conv - mean_c) * lax.rsqrt(var_c + EPS) * channel_norm_gain).astype(jnp.bfloat16)
    attn_group = HEADS * HEAD // N_TP
    conv_group = CH // N_TP
    total = jnp.zeros((rows, D), jnp.float32)
    for group in range(N_TP):
        partial_value = jnp.dot(attn_out[:, group * attn_group:(group + 1) * attn_group].astype(jnp.float32), delta_output_rows[group * attn_group:(group + 1) * attn_group].astype(jnp.float32), preferred_element_type=jnp.float32)
        partial_value = partial_value + jnp.dot(conv_out[:, group * conv_group:(group + 1) * conv_group].astype(jnp.float32), convolution_output_rows[group * conv_group:(group + 1) * conv_group].astype(jnp.float32), preferred_element_type=jnp.float32)
        total = total + rounded(partial_value)
    return total.astype(jnp.bfloat16)

def reference(tokens, input_norm_gain, query_weight, key_weight, value_weight, decay_gate_weight, write_strength_weight, up_weight, gate_half_weight, log_decay_rate, write_strength_bias, decay_spike_added, starting_state, head_norm_gain, convolution_kernel, channel_norm_gain, delta_output_rows, convolution_output_rows):

    def sequence_wise(input_rows):
        sequence_token, sequence_spike, sequence_state = input_rows
        return single_sequence(sequence_token, sequence_spike, sequence_state, input_norm_gain, query_weight, key_weight, value_weight, decay_gate_weight, write_strength_weight, up_weight, gate_half_weight, log_decay_rate, write_strength_bias, head_norm_gain, convolution_kernel, channel_norm_gain, delta_output_rows, convolution_output_rows)
    return lax.map(sequence_wise, (tokens, decay_spike_added, starting_state))
```

```python
import functools

import jax
import jax.numpy as jnp
from jax import lax
from jax.experimental import pallas as pl
from jax.experimental.pallas import tpu as pltpu
from jax.sharding import PartitionSpec as P

HEADS = 8
HEAD = 128
KSIZE = 31
NX = 4
PAD = 32
EPS = 1e-06
MESH = pl.DeviceIdType.MESH
F32 = jnp.float32
BF16 = jnp.bfloat16


def remote(src, dst, send, recv, **where):
    return pltpu.make_async_remote_copy(
        src_ref=src, dst_ref=dst, send_sem=send, recv_sem=recv, device_id=where, device_id_type=MESH
    )


def arrived(ref, sem):
    pltpu.make_async_copy(ref, ref, sem).wait()


def turn(i, n):
    return lax.rem(i + n, n)


def lanes(i):
    return pl.ds(pl.multiple_of(i * HEAD, HEAD), HEAD)


def composer(z, nz):
    quarter = nz // NX
    return lax.div(z, quarter), lax.rem(z, quarter) == quarter // 2


def gather_kernel(
    nz,
    tok_ref,
    q_ref,
    k_ref,
    v_ref,
    up_ref,
    gate_ref,
    do_ref,
    co_ref,
    gain_ref,
    small_ref,
    spike_ref,
    s0_ref,
    proj_ref,
    raw_ref,
    wout_ref,
    spikes_ref,
    start_ref,
    tok,
    normed,
    win,
    p_send,
    p_recv,
    m_send,
    m_recv,
    t_send,
    t_recv,
    c_send,
    c_recv,
    k_send,
    k_recv,
    s_send,
    s_recv,
    local,
):
    z, x, c = lax.axis_index("sp"), lax.axis_index("fs"), lax.axis_index("tp")
    up, down = turn(z + 1, nz), turn(z - 1, nz)
    right, left, over = turn(x + 1, NX), turn(x - 1, NX), turn(x + 2, NX)
    other = 1 - c
    half = nz // 2
    rows = tok_ref.shape[0]
    seq_me, is_composer = composer(z, nz)

    barrier = pltpu.get_barrier_semaphore()
    for where in ({"sp": up}, {"sp": down}, {"fs": right}, {"fs": left}, {"fs": over}, {"tp": other}):
        pl.semaphore_signal(barrier, inc=1, device_id=where, device_id_type=MESH)
    pl.semaphore_wait(barrier, 6)

    own = [w.at[:, lanes(x)] for w in (q_ref, k_ref, v_ref, up_ref, gate_ref)]
    own += [w.at[lanes(x), :] for w in (do_ref, co_ref)]
    count = len(own)

    def slot(src, j):
        if j < 5:
            return win.at[pl.ds(pl.multiple_of(src * HEAD, HEAD), HEAD), pl.ds(j * HEAD, HEAD)]
        return wout_ref.at[src, j - 5]

    for j in range(count):
        remote(own[j], slot(z, j), p_send.at[0, j], p_recv.at[0, j], sp=up).start()
        remote(own[j], slot(z, j), m_send.at[0, j], m_recv.at[0, j], sp=down).start()

    part = rows // 2
    halves = (pl.ds(0, part), pl.ds(part, part))
    for i in range(2):
        src = tok_ref.at[halves[i]]
        dst = tok.at[x, c, halves[i]]
        remote(src, dst, t_send.at[0, i], t_recv.at[0, i], fs=right).start()
        remote(src, dst, t_send.at[1, i], t_recv.at[1, i], fs=left).start()
    own_over = remote(tok_ref, tok.at[x, c], c_send.at[0], c_recv.at[0], tp=other)
    own_over.start()
    spike_copies = [
        remote(spike_ref, spikes_ref.at[x], k_send.at[d - 1], k_recv.at[d - 1], fs=turn(x + d, NX)) for d in (1, 2, 3)
    ]
    for copy in spike_copies:
        copy.start()
    copies = [
        pltpu.make_async_copy(own[j], slot(z, j), local.at[j]) for j in range(count)
    ]
    copies.append(pltpu.make_async_copy(tok_ref, tok.at[x, c], local.at[count]))
    copies.append(pltpu.make_async_copy(spike_ref, spikes_ref.at[x], local.at[count + 1]))
    for copy in copies:
        copy.start()

    @pl.when(is_composer & (x == seq_me))
    def _():
        sends = [
            remote(s0_ref.at[turn(x + d, NX)], start_ref, s_send.at[d - 1], s_recv.at[0], fs=turn(x + d, NX))
            for d in (1, 2, 3)
        ]
        for copy in sends:
            copy.start()
        mine = pltpu.make_async_copy(s0_ref.at[x], start_ref, local.at[count + 2])
        mine.start()
        mine.wait()
        for copy in sends:
            copy.wait_send()

    @pl.when(jnp.logical_not(is_composer))
    def _():
        start_ref[...] = jnp.zeros_like(start_ref)

    def ring(t, _):
        back, fore = turn(z - t, nz), turn(z + t, nz)
        for j in range(count):
            arrived(slot(back, j), p_recv.at[t - 1, j])

            @pl.when((t < half - 1) | (j % 2 == 0))
            def _(j=j):
                remote(slot(back, j), slot(back, j), p_send.at[t, j], p_recv.at[t, j], sp=up).start()

            arrived(slot(fore, j), m_recv.at[t - 1, j])

            @pl.when((t < half - 1) | (j % 2 == 1))
            def _(j=j):
                remote(slot(fore, j), slot(fore, j), m_send.at[t, j], m_recv.at[t, j], sp=down).start()

        return 0

    first = min(3, half - 1)
    second = min(5, half - 1)
    lax.fori_loop(1, first + 1, ring, 0)
    for i in range(2):
        arrived(tok.at[left, c, halves[i]], t_recv.at[0, i])
        arrived(tok.at[right, c, halves[i]], t_recv.at[1, i])
    remote(tok.at[left, c, halves[0]], tok.at[left, c, halves[0]], t_send.at[2, 0], t_recv.at[2, 0], fs=right).start()
    remote(tok.at[right, c, halves[1]], tok.at[right, c, halves[1]], t_send.at[2, 1], t_recv.at[2, 1], fs=left).start()
    remote(tok.at[left, c], tok.at[left, c], c_send.at[1], c_recv.at[1], tp=other).start()
    remote(tok.at[right, c], tok.at[right, c], c_send.at[2], c_recv.at[2], tp=other).start()
    lax.fori_loop(first + 1, second + 1, ring, 0)
    for i in range(2):
        arrived(tok.at[over, c, halves[i]], t_recv.at[2, i])
    remote(tok.at[over, c], tok.at[over, c], c_send.at[3], c_recv.at[3], tp=other).start()
    copies[count].wait()
    for i, where in enumerate((x, left, right, over)):
        arrived(tok.at[where, other], c_recv.at[i])

    features = tok.shape[-1]
    step = 64

    def norm(i, _):
        s = i // (rows // step)
        r = pl.multiple_of(lax.rem(i, rows // step) * step, step)
        a = tok[s, 0, pl.ds(r, step), :].astype(F32)
        b = tok[s, 1, pl.ds(r, step), :].astype(F32)
        total = jnp.sum(a * a, axis=-1, keepdims=True) + jnp.sum(b * b, axis=-1, keepdims=True)
        scale = lax.rsqrt(total * (1.0 / (2 * features)) + EPS)
        at = pl.ds(pl.multiple_of(i * step, step), step)
        normed[at, :features] = (a * scale * gain_ref[:, :features]).astype(BF16)
        normed[at, features:] = (b * scale * gain_ref[:, features:]).astype(BF16)
        return 0

    lax.fori_loop(0, NX * rows // step, norm, 0)
    lax.fori_loop(second + 1, half, ring, 0)
    far = turn(z + half, nz)
    for j in range(count):
        arrived(slot(far, j), (p_recv if j % 2 == 0 else m_recv).at[half - 1, j])
    for j in range(count):
        copies[j].wait()

    def project(s, _):
        at = pl.ds(pl.multiple_of(s * rows, rows), rows)
        tokens = normed[at, :]
        for lo, hi in ((0, 256), (256, 512), (512, 640)):
            proj_ref[at, lo:hi] = jnp.dot(tokens, win[:, lo:hi], preferred_element_type=F32).astype(BF16)
        raw_ref[at, :] = jnp.dot(tokens, small_ref[...], preferred_element_type=F32).astype(BF16)
        return 0

    lax.fori_loop(0, NX, project, 0)

    @pl.when(is_composer & (x != seq_me))
    def _():
        arrived(start_ref, s_recv.at[0])

    copies[count + 1].wait()
    for d in (1, 2, 3):
        arrived(spikes_ref.at[turn(x - d, NX)], k_recv.at[d - 1])
        spike_copies[d - 1].wait_send()

    def drain(t, _):
        for j in range(count):

            @pl.when((t < half - 1) | (j % 2 == 0))
            def _(j=j):
                remote(slot(z, j), slot(z, j), p_send.at[t, j], p_recv.at[t, j], sp=up).wait_send()

            @pl.when((t < half - 1) | (j % 2 == 1))
            def _(j=j):
                remote(slot(z, j), slot(z, j), m_send.at[t, j], m_recv.at[t, j], sp=down).wait_send()

        return 0

    lax.fori_loop(0, half, drain, 0)
    for i in range(2):
        for where, row in ((right, 0), (left, 1), (right, 2)):
            remote(
                tok.at[x, c, halves[i]], tok.at[x, c, halves[i]], t_send.at[row, i], t_recv.at[row, i], fs=where
            ).wait_send()
    for i in range(4):
        remote(tok.at[x, c], tok.at[x, c], c_send.at[i], c_recv.at[i], tp=other).wait_send()


def gathered(nz, tokens, weights, gain, small, spike, start):
    rows, features = tokens.shape
    half = nz // 2
    count = len(weights)
    vmem = pl.BlockSpec(memory_space=pltpu.VMEM)
    dma = pltpu.SemaphoreType.DMA
    return pl.pallas_call(
        functools.partial(gather_kernel, nz),
        name="gather",
        out_shape=(
            jax.ShapeDtypeStruct((NX * rows, 5 * HEAD), BF16),
            jax.ShapeDtypeStruct((NX * rows, HEAD), BF16),
            jax.ShapeDtypeStruct((nz, 2, HEAD, HEAD), BF16),
            jax.ShapeDtypeStruct((NX, *spike.shape), F32),
            jax.ShapeDtypeStruct((HEAD, HEAD), F32),
        ),
        in_specs=[vmem] * (count + 5),
        out_specs=(vmem,) * 5,
        scratch_shapes=[
            pltpu.VMEM((NX, 2, rows, features), BF16),
            pltpu.VMEM((NX * rows, 2 * features), BF16),
            pltpu.VMEM((nz * HEAD, 5 * HEAD), BF16),
            dma((half, count)),
            dma((half, count)),
            dma((half, count)),
            dma((half, count)),
            dma((3, 2)),
            dma((3, 2)),
            dma((4,)),
            dma((4,)),
            dma((3,)),
            dma((3,)),
            dma((3,)),
            dma((1,)),
            dma((count + 3,)),
        ],
        compiler_params=pltpu.CompilerParams(
            collective_id=0, has_side_effects=True, vmem_limit_bytes=56 * 1024 * 1024
        ),
    )(tokens, *weights, gain, small, spike, start)


def dot(a, b):
    return jnp.dot(a.astype(BF16), b.astype(BF16), preferred_element_type=F32)


def dot_t(a, b):
    dims = (((1,), (1,)), ((), ()))
    return lax.dot_general(a.astype(BF16), b.astype(BF16), dims, preferred_element_type=F32)


def dot_of_t(a, b):
    dims = (((0,), (0,)), ((), ()))
    return lax.dot_general(a.astype(BF16), b.astype(BF16), dims, preferred_element_type=F32)


def silu(a):
    return a * jax.nn.sigmoid(a)


def unit_rows(a):
    return a * lax.rsqrt(jnp.sum(a * a, axis=-1, keepdims=True) + EPS)


def unit_lower_inverse(a, row, col):
    size = a.shape[0]
    eye = jnp.where(row == col, 1.0, 0.0)
    inverse = eye - jnp.where((row - col == 1) & (lax.rem(row, 2) == 1), a, 0.0)
    width = 2
    while width < size:
        same = lax.div(row, 2 * width) == lax.div(col, 2 * width)
        block = jnp.where(same & (lax.div(row, width) != lax.div(col, width)), a, 0.0)
        inverse = inverse - dot(dot(inverse, block), inverse)
        width *= 2
    return inverse


def mix_kernel(
    nz,
    proj_ref,
    raw_ref,
    wpart_ref,
    spikes_ref,
    start_ref,
    rate_ref,
    bias_ref,
    head_gain_ref,
    taps_ref,
    channel_gain_ref,
    out_ref,
    base,
    reader,
    map_out,
    map_in,
    states,
    state_in,
    rim_out,
    rim_in,
    extended,
    conv_out,
    conv_all,
    attn_out,
    attn_all,
    wout,
    partial,
    map_send,
    map_recv,
    state_send,
    state_recv,
    rim_sem,
    conv_send,
    conv_recv,
    attn_send,
    attn_recv,
    w_send,
    w_recv,
):
    z, x, c = lax.axis_index("sp"), lax.axis_index("fs"), lax.axis_index("tp")
    right, left, over = turn(x + 1, NX), turn(x - 1, NX), turn(x + 2, NX)
    other = 1 - c
    head = c * NX + x
    rows = proj_ref.shape[0] // NX
    half = nz // 2
    quarter = nz // NX
    seq_me, is_composer = composer(z, nz)
    last = nz - 1

    barrier = pltpu.get_barrier_semaphore()
    for d in range(1, nz):
        pl.semaphore_signal(barrier, inc=1, device_id={"sp": turn(z + d, nz)}, device_id_type=MESH)
    for d in range(NX):
        peer = turn(x + d, NX)
        if d:
            pl.semaphore_signal(barrier, inc=1, device_id={"fs": peer}, device_id_type=MESH)
        pl.semaphore_signal(barrier, inc=1, device_id={"fs": peer, "tp": other}, device_id_type=MESH)

    rate = jnp.exp(jnp.full((1, rows), rate_ref[head], F32))
    bias = bias_ref[head]
    row = lax.broadcasted_iota(jnp.int32, (rows, rows), 0)
    col = lax.broadcasted_iota(jnp.int32, (rows, rows), 1)

    for s in range(NX):
        at = pl.ds(s * rows, rows)
        glu = proj_ref[at, 384:512].astype(F32) * jax.nn.sigmoid(proj_ref[at, 512:640].astype(F32))
        glu = glu.astype(BF16)
        extended[s, pl.ds(PAD, rows), :] = glu.astype(F32)
        rim_out[s] = glu[rows - PAD :]

    def delta(s):
        at = pl.ds(s * rows, rows)
        query = unit_rows(silu(proj_ref[at, 0:128].astype(F32))) * HEAD ** (-0.5)
        keys = unit_rows(silu(proj_ref[at, 128:256].astype(F32)))
        values = silu(proj_ref[at, 256:384].astype(F32))
        raw = raw_ref[at, :]
        pick = lax.broadcasted_iota(jnp.int32, (8, HEAD), 1) == head
        logit = dot_t(jnp.where(pick, 1.0, 0.0), raw)[0:1]
        soft = jnp.maximum(logit, 0.0) + jnp.log1p(jnp.exp(-jnp.abs(logit)))
        log_row = -rate * soft + spikes_ref[s, pl.ds(x, 1), :]
        place = lax.broadcasted_iota(jnp.int32, (rows, HEAD), 1) == HEADS + head
        beta = jnp.sum(jnp.where(place, raw.astype(F32), 0.0), axis=1, keepdims=True)
        beta = jax.nn.sigmoid(beta + bias)
        log_col = jnp.sum(jnp.where(row == col, log_row, 0.0), axis=1, keepdims=True)
        cum_col = jnp.sum(jnp.where(col <= row, log_row, 0.0), axis=1, keepdims=True)
        cum_row = jnp.sum(jnp.where(row <= col, log_col, 0.0), axis=0, keepdims=True)
        total = cum_col[rows - 1 :, :]
        gamma = jnp.where(col <= row, jnp.exp(jnp.minimum(cum_col - cum_row, 0.0)), 0.0)
        grown = jnp.exp(cum_col)
        gram = dot_t(keys, keys)
        a_matrix = jnp.where(col < row, beta * gram * gamma, 0.0)
        inverse = unit_lower_inverse(a_matrix, row, col)
        both = dot(inverse, jnp.concatenate([beta * values, (beta * grown) * keys], axis=1))
        decayed = keys * jnp.exp(total - cum_col)
        mapped = dot_of_t(decayed, both)
        keep = jnp.exp(total)
        keep_hi = keep.astype(BF16).astype(F32)
        rest = keep - keep_hi
        tail = lax.broadcasted_iota(jnp.int32, (16, 2 * HEAD), 0)
        map_out[s, 0:HEAD, :] = mapped.astype(BF16)
        map_out[s, HEAD:, :] = jnp.where(tail < 8, keep_hi, rest).astype(BF16)
        scores = dot_t(query, keys) * gamma
        read = dot(scores, both)
        base[s] = read[:, :HEAD]
        reader[s] = (grown * query - read[:, HEAD:]).astype(BF16)

    def send_map(s):
        owner = s * quarter + quarter // 2

        @pl.when((z != owner) & (z != last))
        def _():
            remote(map_out.at[s], map_in.at[z], map_send.at[s], map_recv.at[z], sp=owner).start()

        @pl.when((z == owner) & (z != last))
        def _():
            pltpu.make_async_copy(map_out.at[s], map_in.at[z], map_recv.at[z]).start()

    delta(0)
    pl.semaphore_wait(barrier, last + 2 * NX - 1)

    @pl.when(z < last)
    def _():
        remote(rim_out, rim_in, rim_sem.at[0], rim_sem.at[1], sp=z + 1).start()

    mine = wpart_ref.at[pl.ds(c * half, half)]
    theirs = wpart_ref.at[pl.ds(other * half, half)]
    own_w = pltpu.make_async_copy(mine, wout.at[head], w_recv.at[9])
    first_w = [
        remote(mine, wout.at[head], w_send.at[0], w_recv.at[0], fs=right),
        remote(theirs, wout.at[head], w_send.at[1], w_recv.at[1], fs=right, tp=other),
        remote(mine, wout.at[head], w_send.at[2], w_recv.at[2], fs=left),
        remote(theirs, wout.at[head], w_send.at[3], w_recv.at[3], fs=left, tp=other),
        remote(theirs, wout.at[head], w_send.at[4], w_recv.at[4], tp=other),
    ]
    own_w.start()
    for copy in first_w:
        copy.start()
    for s in range(1, NX):
        delta(s)
        send_map(s - 1)

    @pl.when(z > 0)
    def _():
        arrived(rim_in, rim_sem.at[1])
        extended[:, 0:PAD, :] = rim_in[...].astype(F32)

    @pl.when(z == 0)
    def _():
        extended[:, 0:PAD, :] = jnp.zeros((NX, PAD, HEAD), F32)

    send_map(NX - 1)

    piece = 64
    pieces = rows // piece
    taps = taps_ref[:, lanes(head)]

    for s in range(NX):
        for r in range(pieces):
            conv = jnp.zeros((piece, HEAD), F32)
            for tap in range(KSIZE):
                conv = conv + taps[tap : tap + 1] * extended[s, pl.ds(r * piece + tap + PAD - KSIZE + 1, piece), :]
            conv_out[s, pl.ds(r * piece, piece), :] = conv.astype(BF16)

    @pl.when(is_composer)
    def _():

        def give(i):
            @pl.when(i != z)
            def _():
                remote(states.at[i], state_in.at[seq_me], state_send.at[i], state_recv.at[seq_me], sp=i).start()

            @pl.when(i == z)
            def _():
                pltpu.make_async_copy(states.at[i], state_in.at[seq_me], state_recv.at[seq_me]).start()

        def advance(i, state):
            states[i] = state.astype(BF16)
            arrived(map_in.at[i], map_recv.at[i])
            block = map_in[i]
            keep = block[HEAD : HEAD + 1, :HEAD].astype(F32) + block[HEAD + 8 : HEAD + 9, :HEAD].astype(F32)
            high = state.astype(BF16)
            low = state - high.astype(F32)
            reduce = dot(block[:HEAD, HEAD:], high) + dot(block[:HEAD, HEAD:], low)
            result = keep * state - reduce + block[:HEAD, :HEAD].astype(F32)
            give(i)
            return result

        states[last] = lax.fori_loop(0, last, advance, start_ref[...]).astype(BF16)

    def exchange(src, dst, send, recv):
        for d in range(NX):
            s = turn(x + d, NX)
            if d == 0:
                pltpu.make_async_copy(src.at[s], dst.at[:, lanes(head)], recv.at[0]).start()
            else:
                remote(src.at[s], dst.at[:, lanes(head)], send.at[d], recv.at[d], fs=s).start()
            remote(src.at[s], dst.at[:, lanes(head)], send.at[NX + d], recv.at[NX + d], fs=s, tp=other).start()

    def exchanged(src, dst, send, recv):
        for d in range(NX):
            source = turn(x - d, NX)
            arrived(dst.at[:, lanes(c * NX + source)], recv.at[d])
            arrived(dst.at[:, lanes(other * NX + source)], recv.at[NX + d])
            if d:
                remote(src.at[0], dst.at[:, lanes(head)], send.at[d], recv.at[d], fs=right).wait_send()
            remote(src.at[0], dst.at[:, lanes(head)], send.at[NX + d], recv.at[NX + d], fs=right).wait_send()

    exchange(conv_out, conv_all, conv_send, conv_recv)

    @pl.when(is_composer)
    def _():
        @pl.when(z != last)
        def _():
            remote(states.at[last], state_in.at[seq_me], state_send.at[last], state_recv.at[seq_me], sp=last).start()

        @pl.when(z == last)
        def _():
            pltpu.make_async_copy(states.at[last], state_in.at[seq_me], state_recv.at[seq_me]).start()

    w_arrivals = ((c, left, 0), (other, left, 1), (c, right, 2), (other, right, 3))
    near, rest = pl.ds(0, half // 2), pl.ds(half // 2, half - half // 2)
    for core, source, i in w_arrivals:
        held = wout.at[core * NX + source]
        arrived(held, w_recv.at[i])
        part = held.at[near] if i < 2 else held.at[rest]
        remote(part, part, w_send.at[5 + i], w_recv.at[5 + i], fs=right if i < 2 else left).start()

    head_gain = head_gain_ref[...]
    for s in range(NX):
        arrived(state_in.at[s], state_recv.at[s])
        attn = base[s] + jnp.dot(reader[s], state_in[s], preferred_element_type=F32)
        scale = lax.rsqrt(jnp.mean(attn * attn, axis=-1, keepdims=True) + EPS)
        attn_out[s] = (attn * scale * head_gain).astype(BF16)

    exchange(attn_out, attn_all, attn_send, attn_recv)
    exchanged(conv_out, conv_all, conv_send, conv_recv)

    def channel_norm(i, _):
        at = pl.ds(pl.multiple_of(i * 64, 64), 64)
        conv = conv_all[at, :].astype(F32)
        mean = jnp.mean(conv, axis=-1, keepdims=True)
        var = jnp.mean(conv * conv, axis=-1, keepdims=True) - mean * mean
        conv_all[at, :] = silu((conv - mean) * lax.rsqrt(var + EPS) * channel_gain_ref[...]).astype(BF16)
        return 0

    lax.fori_loop(0, rows // 64, channel_norm, 0)
    arrived(wout.at[head], w_recv.at[9])
    arrived(wout.at[other * NX + x], w_recv.at[4])
    for core, i in ((c, 5), (other, 6), (c, 7), (other, 8)):
        held = wout.at[core * NX + over]
        arrived(held.at[near] if i < 7 else held.at[rest], w_recv.at[i])

    def weights(j, kind):
        return wout[:, j, kind].reshape(HEADS * HEAD, HEAD)

    def conv_part(j, _):
        partial[j] = jnp.dot(conv_all[...], weights(j, 1), preferred_element_type=F32)
        return 0

    lax.fori_loop(0, half, conv_part, 0)
    exchanged(attn_out, attn_all, attn_send, attn_recv)

    def attn_part(j, _):
        total = partial[j] + jnp.dot(attn_all[...], weights(j, 0), preferred_element_type=F32)
        out_ref[:, lanes(j)] = total.astype(BF16)
        return 0

    lax.fori_loop(0, half, attn_part, 0)

    for s in range(NX):

        @pl.when((z != s * quarter + quarter // 2) & (z != last))
        def _(s=s):
            remote(map_out.at[s], map_in.at[z], map_send.at[s], map_recv.at[z], sp=0).wait_send()

    @pl.when(z < last)
    def _():
        remote(rim_out, rim_in, rim_sem.at[0], rim_sem.at[1], sp=z + 1).wait_send()

    @pl.when(is_composer)
    def _():
        def drain(i, _):
            @pl.when(i != z)
            def _():
                remote(states.at[i], state_in.at[seq_me], state_send.at[i], state_recv.at[seq_me], sp=i).wait_send()

            return 0

        lax.fori_loop(0, nz, drain, 0)

    for copy in first_w:
        copy.wait_send()
    for core, source, i in w_arrivals:
        held = wout.at[core * NX + source]
        part = held.at[near] if i < 2 else held.at[rest]
        remote(part, part, w_send.at[5 + i], w_recv.at[5 + i], fs=right).wait_send()


def mixed_tokens(nz, rows, proj, raw, wpart, spikes, start, rate, bias, head_gain, taps, channel_gain):
    half = nz // 2
    vmem = pl.BlockSpec(memory_space=pltpu.VMEM)
    smem = pl.BlockSpec(memory_space=pltpu.SMEM)
    dma = pltpu.SemaphoreType.DMA
    width = HEADS * HEAD
    return pl.pallas_call(
        functools.partial(mix_kernel, nz),
        name="mix",
        out_shape=jax.ShapeDtypeStruct((rows, half * HEAD), BF16),
        in_specs=[vmem] * 5 + [smem] * 2 + [vmem] * 3,
        out_specs=vmem,
        scratch_shapes=[
            pltpu.VMEM((NX, rows, HEAD), F32),
            pltpu.VMEM((NX, rows, HEAD), BF16),
            pltpu.VMEM((NX, HEAD + 16, 2 * HEAD), BF16),
            pltpu.VMEM((nz, HEAD + 16, 2 * HEAD), BF16),
            pltpu.VMEM((nz, HEAD, HEAD), BF16),
            pltpu.VMEM((NX, HEAD, HEAD), BF16),
            pltpu.VMEM((NX, PAD, HEAD), BF16),
            pltpu.VMEM((NX, PAD, HEAD), BF16),
            pltpu.VMEM((NX, PAD + rows, HEAD), F32),
            pltpu.VMEM((NX, rows, HEAD), BF16),
            pltpu.VMEM((rows, width), BF16),
            pltpu.VMEM((NX, rows, HEAD), BF16),
            pltpu.VMEM((rows, width), BF16),
            pltpu.VMEM((HEADS, half, 2, HEAD, HEAD), BF16),
            pltpu.VMEM((half, rows, HEAD), F32),
            dma((NX,)),
            dma((nz,)),
            dma((nz,)),
            dma((NX,)),
            dma((2,)),
            dma((2 * NX,)),
            dma((2 * NX,)),
            dma((2 * NX,)),
            dma((2 * NX,)),
            dma((9,)),
            dma((10,)),
        ],
        compiler_params=pltpu.CompilerParams(
            collective_id=1, has_side_effects=True, vmem_limit_bytes=56 * 1024 * 1024
        ),
    )(proj, raw, wpart, spikes, start, rate, bias, head_gain, taps, channel_gain)


def on_device(
    nz,
    tokens,
    input_norm_gain,
    query_weight,
    key_weight,
    value_weight,
    decay_gate_weight,
    write_strength_weight,
    up_weight,
    gate_half_weight,
    log_decay_rate,
    write_strength_bias,
    decay_spike_added,
    starting_state,
    head_norm_gain,
    convolution_kernel,
    channel_norm_gain,
    delta_output_rows,
    convolution_output_rows,
):
    rows = tokens.shape[1]
    small = jnp.concatenate([decay_gate_weight, write_strength_weight], axis=1)
    small = jnp.pad(small, ((0, 0), (0, HEAD - small.shape[1])))
    spike = jnp.pad(decay_spike_added[0].T, ((0, 8 - NX), (0, 0)))
    weights = (
        query_weight,
        key_weight,
        value_weight,
        up_weight,
        gate_half_weight,
        delta_output_rows,
        convolution_output_rows,
    )
    proj, raw, wpart, spikes, start = gathered(
        nz, tokens[0], weights, input_norm_gain[None], small, spike, starting_state[0]
    )
    mixed = mixed_tokens(
        nz,
        rows,
        proj,
        raw,
        wpart,
        spikes,
        start,
        log_decay_rate,
        write_strength_bias,
        head_norm_gain[None],
        convolution_kernel,
        channel_norm_gain[None],
    )
    return mixed[None]


def solution(mesh):
    return jax.shard_map(
        functools.partial(on_device, mesh.shape["sp"]),
        mesh=mesh,
        in_specs=(
            P(("grp", "fs"), "sp", "tp"),
            P(),
            P("sp", "tp"),
            P("sp", "tp"),
            P("sp", "tp"),
            P(),
            P(),
            P("sp", "tp"),
            P("sp", "tp"),
            P(),
            P(),
            P(("grp", "fs"), "sp", "tp"),
            P(("grp", "fs"), "tp", None, None),
            P(),
            P(),
            P(),
            P("tp", "sp"),
            P("tp", "sp"),
        ),
        out_specs=P(("grp", "fs"), "sp", "tp"),
        check_vma=False,
    )
```

```python
import functools

import jax
import jax.numpy as jnp
from jax import lax
from jax.experimental import pallas as pl
from jax.experimental.pallas import tpu as pltpu
from jax.sharding import PartitionSpec as P

HEADS = 8
HEAD = 128
KSIZE = 31
NX = 4
PAD = 32
EPS = 1e-06
MESH = pl.DeviceIdType.MESH
F32 = jnp.float32
BF16 = jnp.bfloat16


def remote(src, dst, send, recv, **where):
    return pltpu.make_async_remote_copy(
        src_ref=src, dst_ref=dst, send_sem=send, recv_sem=recv, device_id=where, device_id_type=MESH
    )


def arrived(ref, sem):
    pltpu.make_async_copy(ref, ref, sem).wait()


def turn(i, n):
    return lax.rem(i + n, n)


def lanes(i):
    return pl.ds(pl.multiple_of(i * HEAD, HEAD), HEAD)


def composer(z, nz):
    quarter = nz // NX
    return lax.div(z, quarter), lax.rem(z, quarter) == quarter // 2


def dot(a, b):
    return jnp.dot(a.astype(BF16), b.astype(BF16), preferred_element_type=F32)


def dot_t(a, b):
    dims = (((1,), (1,)), ((), ()))
    return lax.dot_general(a.astype(BF16), b.astype(BF16), dims, preferred_element_type=F32)


def dot_of_t(a, b):
    dims = (((0,), (0,)), ((), ()))
    return lax.dot_general(a.astype(BF16), b.astype(BF16), dims, preferred_element_type=F32)


def silu(a):
    return a * jax.nn.sigmoid(a)


def unit_rows(a):
    return a * lax.rsqrt(jnp.sum(a * a, axis=-1, keepdims=True) + EPS)


def unit_lower_inverse(a, row, col):
    size = a.shape[0]
    eye = jnp.where(row == col, 1.0, 0.0)
    inverse = eye - jnp.where((row - col == 1) & (lax.rem(row, 2) == 1), a, 0.0)
    width = 2
    while width < size:
        same = lax.div(row, 2 * width) == lax.div(col, 2 * width)
        block = jnp.where(same & (lax.div(row, width) != lax.div(col, width)), a, 0.0)
        inverse = inverse - dot(dot(inverse, block), inverse)
        width *= 2
    return inverse


def kernel(
    nz,
    paired,
    tok_ref,
    k_ref,
    v_ref,
    q_ref,
    up_ref,
    gate_ref,
    do_ref,
    co_ref,
    gain_ref,
    decay_ref,
    strength_ref,
    spike_ref,
    s0_ref,
    rate_ref,
    bias_ref,
    head_gain_ref,
    taps_ref,
    channel_gain_ref,
    out_ref,
    tok,
    normed,
    win,
    wring,
    wout,
    spike_rows,
    spikes,
    start,
    keys_at,
    gammas,
    growth,
    solved,
    base,
    reader,
    map_out,
    map_in,
    states,
    state_in,
    rim_out,
    rim_in,
    extended,
    conv_out,
    conv_all,
    attn_out,
    attn_all,
    partial,
    ring_send,
    ring_recv,
    y_send,
    y_recv,
    near_send,
    near_recv,
    far_send,
    far_recv,
    own_send,
    own_recv,
    t_send,
    t_recv,
    c_send,
    c_recv,
    k_send,
    k_recv,
    s_send,
    s_recv,
    local,
    map_send,
    map_recv,
    state_send,
    state_recv,
    rim_sem,
    conv_send,
    conv_recv,
    attn_send,
    attn_recv,
):
    z, x, c = lax.axis_index("sp"), lax.axis_index("fs"), lax.axis_index("tp")
    up, down = turn(z + 1, nz), turn(z - 1, nz)
    right, left, over = turn(x + 1, NX), turn(x - 1, NX), turn(x + 2, NX)
    other = 1 - c
    head = c * NX + x
    half = nz // 2
    quarter = nz // NX
    last = nz - 1
    rows, features = tok_ref.shape
    seq_me, is_composer = composer(z, nz)
    group = lax.axis_index("grp")
    parity = lax.rem(group, 2)
    partner = group + 1 - 2 * parity

    neighbours = [{"sp": up}, {"sp": down}, {"fs": right}, {"fs": left}, {"fs": over}, {"tp": other}]
    neighbours += [{"fs": right, "tp": other}, {"fs": left, "tp": other}, {"fs": over, "tp": other}]
    if paired:
        neighbours.append({"grp": partner})
    barrier = pltpu.get_barrier_semaphore()
    for where in neighbours:
        pl.semaphore_signal(barrier, inc=1, device_id=where, device_id_type=MESH)

    def block_of(src, j):
        return win.at[pl.ds(pl.multiple_of(src * HEAD, HEAD), HEAD), lanes(j)]

    own = [w.at[:, lanes(x)] for w in (k_ref, v_ref, q_ref, up_ref, gate_ref)]
    own += [w.at[lanes(x), :] for w in (do_ref, co_ref)]
    own_at = [block_of(z, j) for j in range(5)] + [wring.at[z, j] for j in range(2)]
    copies = [pltpu.make_async_copy(a, b, local.at[j]) for j, (a, b) in enumerate(zip(own, own_at))]
    copies.append(pltpu.make_async_copy(tok_ref, tok.at[x, c], local.at[7]))
    for copy in copies:
        copy.start()

    row = lax.broadcasted_iota(jnp.int32, (rows, rows), 0)
    col = lax.broadcasted_iota(jnp.int32, (rows, rows), 1)

    def to_row(column):
        return jnp.sum(jnp.where(row == col, column, 0.0), axis=0, keepdims=True)

    def to_column(line):
        return jnp.sum(jnp.where(row == col, line, 0.0), axis=1, keepdims=True)

    spike = spike_ref[...]
    spike_rows[...] = jnp.zeros_like(spike_rows)
    for i in range(NX):
        spike_rows[i : i + 1, :] = to_row(spike[:, i : i + 1])

    if paired:
        places = [lambda src, j=j: block_of(src, j) for j in range(3)]
        places += [lambda src: block_of(src, 3 + parity), lambda src: wring.at[src, parity]]
        shared = {3: 0, 4: 1}
    else:
        places = [lambda src, j=j: block_of(src, j) for j in range(5)]
        places += [lambda src, j=j: wring.at[src, j] for j in range(2)]
        shared = {}
    count = len(places)

    def hop(t, pos, way, src):
        ref = places[pos](src)
        sem = ring_send.at[way, lax.rem(t, 2), pos]
        return remote(ref, ref, sem, ring_recv.at[way, t, pos], sp=up if way == 0 else down)

    def spread(src):
        core, zz = lax.div(src, half), lax.rem(src, half)
        other_core = core + c - 2 * core * c
        piece, target = wring.at[src], wout.at[head, zz]
        remote(piece, target, near_send.at[0, src], near_recv.at[0, other_core, zz], fs=right, tp=core).start()
        remote(piece, target, near_send.at[1, src], near_recv.at[1, other_core, zz], fs=left, tp=core).start()

        @pl.when(other_core == 0)
        def _():
            pltpu.make_async_copy(piece, target, own_recv.at[0, zz]).start()

        @pl.when(other_core == 1)
        def _():
            remote(piece, target, own_send.at[zz], own_recv.at[1, zz], tp=other).start()

    pl.semaphore_wait(barrier, len(neighbours))
    for j in range(7):
        copies[j].wait()
    for pos in range(count):
        hop(0, pos, 0, z).start()
        hop(0, pos, 1, z).start()

    part = rows // 2
    halves = (pl.ds(0, part), pl.ds(part, part))
    for i in range(2):
        src = tok_ref.at[halves[i]]
        dst = tok.at[x, c, halves[i]]
        remote(src, dst, t_send.at[0, i], t_recv.at[0, i], fs=right).start()
        remote(src, dst, t_send.at[1, i], t_recv.at[1, i], fs=left).start()
    remote(tok_ref, tok.at[x, c], c_send.at[0], c_recv.at[0], tp=other).start()
    spike_copies = [
        remote(spike_rows, spikes.at[x], k_send.at[d - 1], k_recv.at[d - 1], fs=turn(x + d, NX)) for d in (1, 2, 3)
    ]
    for copy in spike_copies:
        copy.start()
    spike_own = pltpu.make_async_copy(spike_rows, spikes.at[x], local.at[8])
    spike_own.start()

    start_sends = [
        remote(s0_ref.at[turn(x + d, NX)], start, s_send.at[d - 1], s_recv.at[0], fs=turn(x + d, NX)) for d in (1, 2, 3)
    ]

    @pl.when(is_composer & (x == seq_me))
    def _():
        for copy in start_sends:
            copy.start()
        pltpu.make_async_copy(s0_ref.at[x], start, s_recv.at[0]).start()

    spread(z)

    step = 64

    def norm(s):
        def some(i, _):
            r = pl.ds(pl.multiple_of(i * step, step), step)
            a = tok[s, 0, r, :].astype(F32)
            b = tok[s, 1, r, :].astype(F32)
            total = jnp.sum(a * a, axis=-1, keepdims=True) + jnp.sum(b * b, axis=-1, keepdims=True)
            scale = lax.rsqrt(total * (1.0 / (2 * features)) + EPS)
            at = pl.ds(pl.multiple_of(s * rows + i * step, step), step)
            normed[at, :features] = (a * scale * gain_ref[:, :features]).astype(BF16)
            normed[at, features:] = (b * scale * gain_ref[:, features:]).astype(BF16)
            return 0

        lax.fori_loop(0, rows // step, some, 0)

    def pass_on(i, src):
        remote(tok.at[src, c], tok.at[src, c], c_send.at[i], c_recv.at[i], tp=other).start()

    def tokens_near():
        for i in range(2):
            arrived(tok.at[left, c, halves[i]], t_recv.at[0, i])
            arrived(tok.at[right, c, halves[i]], t_recv.at[1, i])
        a, b = tok.at[left, c, halves[0]], tok.at[right, c, halves[1]]
        remote(a, a, t_send.at[2, 0], t_recv.at[2, 0], fs=right).start()
        remote(b, b, t_send.at[2, 1], t_recv.at[2, 1], fs=left).start()
        pass_on(1, left)
        pass_on(2, right)

    def norm_own():
        copies[7].wait()
        arrived(tok.at[x, other], c_recv.at[0])
        norm(x)

    def norm_near(i, src):
        arrived(tok.at[src, other], c_recv.at[i])
        norm(src)

    def tokens_far():
        for i in range(2):
            arrived(tok.at[over, c, halves[i]], t_recv.at[2, i])
        pass_on(3, over)

    hooks = (
        (2, norm_own),
        (4, tokens_near),
        (5, lambda: norm_near(1, left)),
        (6, lambda: norm_near(2, right)),
        (6, tokens_far),
    )

    def ring(t, _):
        back, fore = turn(z - t, nz), turn(z + t, nz)
        for pos in range(count):
            for way, src in ((0, back), (1, fore)):
                arrived(places[pos](src), ring_recv.at[way, t - 1, pos])

                @pl.when(t >= 2)
                def _(pos=pos, way=way):
                    hop(t, pos, way, z).wait_send()

                @pl.when((t < half - 1) | (pos % 2 == way))
                def _(pos=pos, way=way, src=src):
                    hop(t, pos, way, src).start()

                if pos in shared:
                    ref = places[pos](src)
                    i = shared[pos]
                    remote(ref, ref, y_send.at[src, i], y_recv.at[src, i], grp=partner).start()

        @pl.when(t >= 2)
        def _():
            for src in (turn(z - t + 1, nz), turn(z + t - 1, nz)):
                if paired:
                    arrived(wring.at[src, 1 - parity], y_recv.at[src, 1])
                spread(src)

        for when, task in hooks:
            pl.when(t == min(when, half - 1))(task)
        return 0

    lax.fori_loop(1, half, ring, 0)
    far = turn(z + half, nz)
    for pos in range(count):
        arrived(places[pos](far), ring_recv.at[pos % 2, half - 1, pos])
        if pos in shared:
            ref = places[pos](far)
            i = shared[pos]
            remote(ref, ref, y_send.at[far, i], y_recv.at[far, i], grp=partner).start()
    norm_near(3, over)

    for d in (1, 2, 3):
        arrived(spikes.at[turn(x - d, NX)], k_recv.at[d - 1])
    spike_own.wait()

    rate = jnp.exp(jnp.full((rows, 1), rate_ref[head], F32))
    bias = bias_ref[head]
    lane = lax.broadcasted_iota(jnp.int32, (rows, HEADS), 1)

    def delta(s):
        at = pl.ds(s * rows, rows)
        tokens = normed[at, :]
        raw = jnp.dot(tokens, win[:, : 2 * HEAD], preferred_element_type=F32).astype(BF16).astype(F32)
        keys = unit_rows(silu(raw[:, :HEAD]))
        values = silu(raw[:, HEAD:])

        def gate(ref):
            both = jnp.dot(tokens, ref[...], preferred_element_type=F32).astype(BF16).astype(F32)
            return jnp.sum(jnp.where(lane == head, both, 0.0), axis=1, keepdims=True)

        logit = gate(decay_ref)
        beta = jax.nn.sigmoid(gate(strength_ref) + bias)
        soft = jnp.maximum(logit, 0.0) + jnp.log1p(jnp.exp(-jnp.abs(logit)))
        log_col = to_column(spikes[s, pl.ds(x, 1), :]) - rate * soft
        log_row = to_row(log_col)
        cum_col = jnp.sum(jnp.where(col <= row, log_row, 0.0), axis=1, keepdims=True)
        cum_row = jnp.sum(jnp.where(row <= col, log_col, 0.0), axis=0, keepdims=True)
        total = cum_col[rows - 1 :, :]
        gamma = jnp.where(col <= row, jnp.exp(jnp.minimum(cum_col - cum_row, 0.0)), 0.0)
        grown = jnp.exp(cum_col)
        a_matrix = jnp.where(col < row, beta * dot_t(keys, keys) * gamma, 0.0)
        inverse = unit_lower_inverse(a_matrix, row, col)
        both = dot(inverse, jnp.concatenate([beta * values, (beta * grown) * keys], axis=1)).astype(BF16)
        mapped = dot_of_t(keys * jnp.exp(total - cum_col), both)
        keep = jnp.exp(total)
        keep_hi = keep.astype(BF16).astype(F32)
        tail = lax.broadcasted_iota(jnp.int32, (16, 2 * HEAD), 0)
        map_out[s, 0:HEAD, :] = mapped.astype(BF16)
        map_out[s, HEAD:, :] = jnp.where(tail < 8, keep_hi, keep - keep_hi).astype(BF16)
        keys_at[s] = keys.astype(BF16)
        gammas[s] = gamma
        growth[s] = jnp.broadcast_to(grown, (rows, HEAD))
        solved[s] = both

    def send_map(s):
        owner = s * quarter + quarter // 2

        @pl.when((z != owner) & (z != last))
        def _():
            remote(map_out.at[s], map_in.at[z], map_send.at[s], map_recv.at[z], sp=owner).start()

        @pl.when((z == owner) & (z != last))
        def _():
            pltpu.make_async_copy(map_out.at[s], map_in.at[z], map_recv.at[z]).start()

    for s in range(NX):
        delta(s)
        if s:
            send_map(s - 1)

    for src in (turn(z - half + 1, nz), turn(z + half - 1, nz), far):
        if paired:
            arrived(wring.at[src, 1 - parity], y_recv.at[src, 1])
        spread(src)
    send_map(NX - 1)
    if paired:

        def shared_in(d, _):
            src = turn(z + d, nz)
            arrived(block_of(src, 4 - parity), y_recv.at[src, 0])
            return 0

        lax.fori_loop(1, nz, shared_in, 0)

    def gated(s):
        at = pl.ds(s * rows, rows)
        raw = jnp.dot(normed[at, :], win[:, 3 * HEAD :], preferred_element_type=F32).astype(BF16).astype(F32)
        glu = (raw[:, :HEAD] * jax.nn.sigmoid(raw[:, HEAD:])).astype(BF16)
        extended[s, pl.ds(PAD, rows), :] = glu.astype(F32)
        rim_out[s] = glu[rows - PAD :]

    def reads(s):
        at = pl.ds(s * rows, rows)
        raw = jnp.dot(normed[at, :], win[:, 2 * HEAD : 3 * HEAD], preferred_element_type=F32).astype(BF16).astype(F32)
        query = unit_rows(silu(raw)) * HEAD ** (-0.5)
        scores = dot_t(query, keys_at[s]) * gammas[s]
        read = dot(scores, solved[s])
        base[s] = read[:, :HEAD]
        reader[s] = (growth[s] * query - read[:, HEAD:]).astype(BF16)

    for s in range(NX):
        gated(s)
    reads(0)

    @pl.when(z < last)
    def _():
        remote(rim_out, rim_in, rim_sem.at[0], rim_sem.at[1], sp=z + 1).start()

    for s in range(1, NX):
        reads(s)

    def second(zz, _):
        for rel, core in ((0, c), (1, other)):
            first, again = wout.at[core * NX + left, zz], wout.at[core * NX + right, zz]
            arrived(first, near_recv.at[0, rel, zz])
            remote(first.at[0], first.at[0], far_send.at[0, rel, zz], far_recv.at[0, rel, zz], fs=right).start()
            arrived(again, near_recv.at[1, rel, zz])
            remote(again.at[1], again.at[1], far_send.at[1, rel, zz], far_recv.at[1, rel, zz], fs=left).start()
        return 0

    lax.fori_loop(0, half, second, 0)

    @pl.when(z > 0)
    def _():
        arrived(rim_in, rim_sem.at[1])
        extended[:, 0:PAD, :] = rim_in[...].astype(F32)

    @pl.when(z == 0)
    def _():
        extended[:, 0:PAD, :] = jnp.zeros((NX, PAD, HEAD), F32)

    piece = 64
    taps = taps_ref[:, lanes(head)]
    for s in range(NX):
        for r in range(rows // piece):
            conv = jnp.zeros((piece, HEAD), F32)
            for tap in range(KSIZE):
                conv = conv + taps[tap : tap + 1] * extended[s, pl.ds(r * piece + tap + PAD - KSIZE + 1, piece), :]
            conv_out[s, pl.ds(r * piece, piece), :] = conv.astype(BF16)

    def give(i):
        @pl.when(i != z)
        def _():
            remote(states.at[i], state_in.at[seq_me], state_send.at[i], state_recv.at[seq_me], sp=i).start()

        @pl.when(i == z)
        def _():
            pltpu.make_async_copy(states.at[i], state_in.at[seq_me], state_recv.at[seq_me]).start()

    @pl.when(is_composer)
    def _():
        arrived(start, s_recv.at[0])

        def advance(i, state):
            states[i] = state.astype(BF16)
            arrived(map_in.at[i], map_recv.at[i])
            block = map_in[i]
            keep = block[HEAD : HEAD + 1, :HEAD].astype(F32) + block[HEAD + 8 : HEAD + 9, :HEAD].astype(F32)
            high = state.astype(BF16)
            low = state - high.astype(F32)
            reduce = dot(block[:HEAD, HEAD:], high) + dot(block[:HEAD, HEAD:], low)
            result = keep * state - reduce + block[:HEAD, :HEAD].astype(F32)
            give(i)
            return result

        states[last] = lax.fori_loop(0, last, advance, start[...]).astype(BF16)

    def exchange(src, dst, send, recv):
        for d in range(NX):
            s = turn(x + d, NX)
            if d == 0:
                pltpu.make_async_copy(src.at[s], dst.at[:, lanes(head)], recv.at[0]).start()
            else:
                remote(src.at[s], dst.at[:, lanes(head)], send.at[d], recv.at[d], fs=s).start()
            remote(src.at[s], dst.at[:, lanes(head)], send.at[NX + d], recv.at[NX + d], fs=s, tp=other).start()

    def exchanged(src, dst, send, recv):
        for d in range(NX):
            source = turn(x - d, NX)
            arrived(dst.at[:, lanes(c * NX + source)], recv.at[d])
            arrived(dst.at[:, lanes(other * NX + source)], recv.at[NX + d])
            if d:
                remote(src.at[0], dst.at[:, lanes(head)], send.at[d], recv.at[d], fs=right).wait_send()
            remote(src.at[0], dst.at[:, lanes(head)], send.at[NX + d], recv.at[NX + d], fs=right).wait_send()

    exchange(conv_out, conv_all, conv_send, conv_recv)
    pl.when(is_composer)(lambda: give(last))

    head_gain = head_gain_ref[...]
    for s in range(NX):
        arrived(state_in.at[s], state_recv.at[s])
        attn = base[s] + jnp.dot(reader[s], state_in[s], preferred_element_type=F32)
        scale = lax.rsqrt(jnp.mean(attn * attn, axis=-1, keepdims=True) + EPS)
        attn_out[s] = (attn * scale * head_gain).astype(BF16)

    exchange(attn_out, attn_all, attn_send, attn_recv)
    exchanged(conv_out, conv_all, conv_send, conv_recv)

    def channel_norm(i, _):
        at = pl.ds(pl.multiple_of(i * 64, 64), 64)
        conv = conv_all[at, :].astype(F32)
        mean = jnp.mean(conv, axis=-1, keepdims=True)
        var = jnp.mean(conv * conv, axis=-1, keepdims=True) - mean * mean
        conv_all[at, :] = silu((conv - mean) * lax.rsqrt(var + EPS) * channel_gain_ref[...]).astype(BF16)
        return 0

    lax.fori_loop(0, rows // 64, channel_norm, 0)

    def weights_in(zz, _):
        arrived(wout.at[head, zz], own_recv.at[0, zz])
        arrived(wout.at[other * NX + x, zz], own_recv.at[1, zz])
        for rel, core in ((0, c), (1, other)):
            for kind in range(2):
                arrived(wout.at[core * NX + over, zz, kind], far_recv.at[kind, rel, zz])
        return 0

    lax.fori_loop(0, half, weights_in, 0)

    def weights(j, kind):
        return wout[:, j, kind].reshape(HEADS * HEAD, HEAD)

    def conv_part(j, _):
        partial[j] = jnp.dot(conv_all[...], weights(j, 1), preferred_element_type=F32)
        return 0

    lax.fori_loop(0, half, conv_part, 0)
    exchanged(attn_out, attn_all, attn_send, attn_recv)

    def attn_part(j, _):
        total = partial[j] + jnp.dot(attn_all[...], weights(j, 0), preferred_element_type=F32)
        out_ref[:, lanes(j)] = total.astype(BF16)
        return 0

    lax.fori_loop(0, half, attn_part, 0)

    for pos in range(count):
        for way in range(2):
            if half > 1:
                hop(half - 2, pos, way, z).wait_send()
            if pos % 2 == way:
                hop(half - 1, pos, way, z).wait_send()
    for i in range(2):
        for where, line in ((right, 0), (left, 1), (right, 2)):
            ref = tok.at[x, c, halves[i]]
            remote(ref, ref, t_send.at[line, i], t_recv.at[line, i], fs=where).wait_send()
    for i in range(4):
        remote(tok.at[x, c], tok.at[x, c], c_send.at[i], c_recv.at[i], tp=other).wait_send()
    for copy in spike_copies:
        copy.wait_send()

    @pl.when(is_composer & (x == seq_me))
    def _():
        for copy in start_sends:
            copy.wait_send()

    def drain(i, _):
        for way in range(2):
            remote(wring.at[i], wout.at[head, 0], near_send.at[way, i], near_recv.at[way, 0, 0], fs=right).wait_send()
        if paired:

            @pl.when(i != z)
            def _():
                a = block_of(i, 3)
                remote(a, a, y_send.at[i, 0], y_recv.at[i, 0], grp=partner).wait_send()
                b = wring.at[i, 0]
                remote(b, b, y_send.at[i, 1], y_recv.at[i, 1], grp=partner).wait_send()

        @pl.when(is_composer & (i != z))
        def _():
            remote(states.at[i], state_in.at[seq_me], state_send.at[i], state_recv.at[seq_me], sp=i).wait_send()

        return 0

    lax.fori_loop(0, nz, drain, 0)

    def drain_half(zz, _):
        remote(wring.at[0], wout.at[head, zz], own_send.at[zz], own_recv.at[1, zz], tp=other).wait_send()
        for way in range(2):
            for rel in range(2):
                ref = wout.at[head, zz, 0]
                remote(ref, ref, far_send.at[way, rel, zz], far_recv.at[way, rel, zz], fs=right).wait_send()
        return 0

    lax.fori_loop(0, half, drain_half, 0)
    for s in range(NX):

        @pl.when((z != s * quarter + quarter // 2) & (z != last))
        def _(s=s):
            remote(map_out.at[s], map_in.at[z], map_send.at[s], map_recv.at[z], sp=0).wait_send()

    @pl.when(z < last)
    def _():
        remote(rim_out, rim_in, rim_sem.at[0], rim_sem.at[1], sp=z + 1).wait_send()


def mixed_tokens(nz, paired, tokens, *rest):
    rows, features = tokens.shape
    half = nz // 2
    count = 5 if paired else 7
    vmem = pl.BlockSpec(memory_space=pltpu.VMEM)
    smem = pl.BlockSpec(memory_space=pltpu.SMEM)
    dma = pltpu.SemaphoreType.DMA
    width = HEADS * HEAD
    return pl.pallas_call(
        functools.partial(kernel, nz, paired),
        name="mix",
        out_shape=jax.ShapeDtypeStruct((rows, half * HEAD), BF16),
        in_specs=[vmem] * 13 + [smem] * 2 + [vmem] * 3,
        out_specs=vmem,
        scratch_shapes=[
            pltpu.VMEM((NX, 2, rows, features), BF16),
            pltpu.VMEM((NX * rows, 2 * features), BF16),
            pltpu.VMEM((nz * HEAD, 5 * HEAD), BF16),
            pltpu.VMEM((nz, 2, HEAD, HEAD), BF16),
            pltpu.VMEM((HEADS, half, 2, HEAD, HEAD), BF16),
            pltpu.VMEM((8, rows), F32),
            pltpu.VMEM((NX, 8, rows), F32),
            pltpu.VMEM((HEAD, HEAD), F32),
            pltpu.VMEM((NX, rows, HEAD), BF16),
            pltpu.VMEM((NX, rows, rows), F32),
            pltpu.VMEM((NX, rows, HEAD), F32),
            pltpu.VMEM((NX, rows, 2 * HEAD), BF16),
            pltpu.VMEM((NX, rows, HEAD), F32),
            pltpu.VMEM((NX, rows, HEAD), BF16),
            pltpu.VMEM((NX, HEAD + 16, 2 * HEAD), BF16),
            pltpu.VMEM((nz, HEAD + 16, 2 * HEAD), BF16),
            pltpu.VMEM((nz, HEAD, HEAD), BF16),
            pltpu.VMEM((NX, HEAD, HEAD), BF16),
            pltpu.VMEM((NX, PAD, HEAD), BF16),
            pltpu.VMEM((NX, PAD, HEAD), BF16),
            pltpu.VMEM((NX, PAD + rows, HEAD), F32),
            pltpu.VMEM((NX, rows, HEAD), BF16),
            pltpu.VMEM((rows, width), BF16),
            pltpu.VMEM((NX, rows, HEAD), BF16),
            pltpu.VMEM((rows, width), BF16),
            pltpu.VMEM((half, rows, HEAD), F32),
            dma((2, 2, count)),
            dma((2, half, count)),
            dma((nz, 2)),
            dma((nz, 2)),
            dma((2, nz)),
            dma((2, 2, half)),
            dma((2, 2, half)),
            dma((2, 2, half)),
            dma((half,)),
            dma((2, half)),
            dma((3, 2)),
            dma((3, 2)),
            dma((4,)),
            dma((4,)),
            dma((3,)),
            dma((3,)),
            dma((3,)),
            dma((1,)),
            dma((9,)),
            dma((NX,)),
            dma((nz,)),
            dma((nz,)),
            dma((NX,)),
            dma((2,)),
            dma((2 * NX,)),
            dma((2 * NX,)),
            dma((2 * NX,)),
            dma((2 * NX,)),
        ],
        compiler_params=pltpu.CompilerParams(
            collective_id=0, has_side_effects=True, vmem_limit_bytes=60 * 1024 * 1024
        ),
    )(tokens, *rest)


def on_device(
    nz,
    paired,
    tokens,
    input_norm_gain,
    query_weight,
    key_weight,
    value_weight,
    decay_gate_weight,
    write_strength_weight,
    up_weight,
    gate_half_weight,
    log_decay_rate,
    write_strength_bias,
    decay_spike_added,
    starting_state,
    head_norm_gain,
    convolution_kernel,
    channel_norm_gain,
    delta_output_rows,
    convolution_output_rows,
):
    mixed = mixed_tokens(
        nz,
        paired,
        tokens[0],
        key_weight,
        value_weight,
        query_weight,
        up_weight,
        gate_half_weight,
        delta_output_rows,
        convolution_output_rows,
        input_norm_gain[None],
        decay_gate_weight,
        write_strength_weight,
        decay_spike_added[0],
        starting_state[0],
        log_decay_rate,
        write_strength_bias,
        head_norm_gain[None],
        convolution_kernel,
        channel_norm_gain[None],
    )
    return mixed[None]


def solution(mesh):
    return jax.shard_map(
        functools.partial(on_device, mesh.shape["sp"], mesh.shape["grp"] % 2 == 0),
        mesh=mesh,
        in_specs=(
            P(("grp", "fs"), "sp", "tp"),
            P(),
            P("sp", "tp"),
            P("sp", "tp"),
            P("sp", "tp"),
            P(),
            P(),
            P("sp", "tp"),
            P("sp", "tp"),
            P(),
            P(),
            P(("grp", "fs"), "sp", "tp"),
            P(("grp", "fs"), "tp", None, None),
            P(),
            P(),
            P(),
            P("tp", "sp"),
            P("tp", "sp"),
        ),
        out_specs=P(("grp", "fs"), "sp", "tp"),
        check_vma=False,
    )
```

```python
import functools

import jax
import jax.numpy as jnp
from jax import lax
from jax.experimental import pallas as pl
from jax.experimental.pallas import tpu as pltpu
from jax.sharding import PartitionSpec as P

HEADS = 8
HEAD = 128
KSIZE = 31
NX = 4
PAD = 32
EPS = 1e-06
MESH = pl.DeviceIdType.MESH
F32 = jnp.float32
BF16 = jnp.bfloat16


def remote(src, dst, send, recv, **where):
    return pltpu.make_async_remote_copy(
        src_ref=src, dst_ref=dst, send_sem=send, recv_sem=recv, device_id=where, device_id_type=MESH
    )


def arrived(ref, sem):
    pltpu.make_async_copy(ref, ref, sem).wait()


def turn(i, n):
    return lax.rem(i + n, n)


def lanes(i):
    return pl.ds(pl.multiple_of(i * HEAD, HEAD), HEAD)


def composer(z, nz):
    quarter = nz // NX
    return lax.div(z, quarter), lax.rem(z, quarter) == quarter // 2


def dot(a, b):
    return jnp.dot(a.astype(BF16), b.astype(BF16), preferred_element_type=F32)


def dot_t(a, b):
    dims = (((1,), (1,)), ((), ()))
    return lax.dot_general(a.astype(BF16), b.astype(BF16), dims, preferred_element_type=F32)


def dot_of_t(a, b):
    dims = (((0,), (0,)), ((), ()))
    return lax.dot_general(a.astype(BF16), b.astype(BF16), dims, preferred_element_type=F32)


def silu(a):
    return a * jax.nn.sigmoid(a)


def unit_rows(a):
    return a * lax.rsqrt(jnp.sum(a * a, axis=-1, keepdims=True) + EPS)


def unit_lower_inverses(blocks, row, col):
    size = blocks[0].shape[0]
    eye = jnp.where(row == col, 1.0, 0.0)
    below = (row - col == 1) & (lax.rem(row, 2) == 1)
    inverses = [eye - jnp.where(below, a, 0.0) for a in blocks]
    width = 2
    while width < size:
        same = lax.div(row, 2 * width) == lax.div(col, 2 * width)
        mask = same & (lax.div(row, width) != lax.div(col, width))
        steps = [dot(b, jnp.where(mask, a, 0.0)) for a, b in zip(blocks, inverses)]
        inverses = [b - dot(p, b) for p, b in zip(steps, inverses)]
        width *= 2
    return inverses


def kernel(
    nz,
    paired,
    tok_ref,
    k_ref,
    v_ref,
    q_ref,
    up_ref,
    gate_ref,
    do_ref,
    co_ref,
    gain_ref,
    decay_ref,
    strength_ref,
    spike_ref,
    s0_ref,
    rate_ref,
    bias_ref,
    head_gain_ref,
    taps_ref,
    channel_gain_ref,
    out_ref,
    tok,
    normed,
    wbuf,
    wout,
    gates,
    spikes,
    start,
    keys_at,
    gammas,
    growth,
    solved,
    base,
    reader,
    map_out,
    map_in,
    states,
    state_in,
    rim_out,
    rim_in,
    extended,
    conv_out,
    conv_all,
    attn_out,
    attn_all,
    partial,
    ring_send,
    ring_recv,
    y_send,
    y_recv,
    near_send,
    near_recv,
    far_send,
    far_recv,
    own_send,
    own_recv,
    t_send,
    t_recv,
    c_send,
    c_recv,
    k_send,
    k_recv,
    s_send,
    s_recv,
    local,
    map_send,
    map_recv,
    state_send,
    state_recv,
    rim_sem,
    conv_send,
    conv_recv,
    attn_send,
    attn_recv,
):
    z, x, c = lax.axis_index("sp"), lax.axis_index("fs"), lax.axis_index("tp")
    up, down = turn(z + 1, nz), turn(z - 1, nz)
    right, left, over = turn(x + 1, NX), turn(x - 1, NX), turn(x + 2, NX)
    other = 1 - c
    head = c * NX + x
    half = nz // 2
    quarter = nz // NX
    last = nz - 1
    rows, features = tok_ref.shape
    seq_me, is_composer = composer(z, nz)
    group = lax.axis_index("grp")
    parity = lax.rem(group, 2)
    partner = group + 1 - 2 * parity

    neighbours = [{"sp": up}, {"sp": down}, {"fs": right}, {"fs": left}, {"fs": over}, {"tp": other}]
    neighbours += [{"fs": right, "tp": other}, {"fs": left, "tp": other}, {"fs": over, "tp": other}]
    if paired:
        neighbours.append({"grp": partner})
    barrier = pltpu.get_barrier_semaphore()
    for where in neighbours:
        pl.semaphore_signal(barrier, inc=1, device_id=where, device_id_type=MESH)

    own = [w.at[:, lanes(x)] for w in (k_ref, v_ref, q_ref, up_ref, gate_ref)]
    own += [w.at[lanes(x), :] for w in (do_ref, co_ref)]
    copies = [pltpu.make_async_copy(a, wbuf.at[z, j], local.at[j]) for j, a in enumerate(own)]
    copies.append(pltpu.make_async_copy(tok_ref, tok.at[x, c], local.at[7]))
    for copy in copies:
        copy.start()

    row = lax.broadcasted_iota(jnp.int32, (rows, rows), 0)
    col = lax.broadcasted_iota(jnp.int32, (rows, rows), 1)

    def to_row(column):
        return jnp.sum(jnp.where(row == col, column, 0.0), axis=0, keepdims=True)

    def to_column(line):
        return jnp.sum(jnp.where(row == col, line, 0.0), axis=1, keepdims=True)

    if paired:
        chunks, shared = [0, 1, 2, 3 + parity, 5 + parity], (3, 4)
    else:
        chunks, shared = list(range(7)), ()
    count = len(chunks)

    def hop(t, pos, way, src):
        ref = wbuf.at[src, chunks[pos]]
        return remote(ref, ref, ring_send.at[way, t, pos], ring_recv.at[way, t, pos], sp=up if way == 0 else down)

    def to_partner(src, i):
        ref = wbuf.at[src, chunks[shared[i]]]
        return remote(ref, ref, y_send.at[src, i], y_recv.at[src, i], grp=partner)

    def whole_piece(src):
        if paired:
            arrived(wbuf.at[src, 6 - parity], y_recv.at[src, 1])

    def spread(src):
        core, zz = lax.div(src, half), lax.rem(src, half)
        other_core = core + c - 2 * core * c
        piece, target = wbuf.at[src, pl.ds(5, 2)], wout.at[head, zz]
        remote(piece, target, near_send.at[0, src], near_recv.at[0, other_core, zz], fs=right, tp=core).start()
        remote(piece, target, near_send.at[1, src], near_recv.at[1, other_core, zz], fs=left, tp=core).start()

        @pl.when(other_core == 0)
        def _():
            pltpu.make_async_copy(piece, target, own_recv.at[0, zz]).start()

        @pl.when(other_core == 1)
        def _():
            remote(piece, target, own_send.at[zz], own_recv.at[1, zz], tp=other).start()

    pl.semaphore_wait(barrier, len(neighbours))
    for j in range(7):
        copies[j].wait()
    for pos in range(count):
        hop(0, pos, 0, z).start()
        hop(0, pos, 1, z).start()

    part = rows // 2
    halves = (pl.ds(0, part), pl.ds(part, part))
    for i in range(2):
        src = tok_ref.at[halves[i]]
        dst = tok.at[x, c, halves[i]]
        remote(src, dst, t_send.at[0, i], t_recv.at[0, i], fs=right).start()
        remote(src, dst, t_send.at[1, i], t_recv.at[1, i], fs=left).start()
    remote(tok_ref, tok.at[x, c], c_send.at[0], c_recv.at[0], tp=other).start()
    spike_copies = [
        remote(spike_ref, spikes.at[x], k_send.at[d - 1], k_recv.at[d - 1], fs=turn(x + d, NX)) for d in (1, 2, 3)
    ]
    for copy in spike_copies:
        copy.start()
    spike_own = pltpu.make_async_copy(spike_ref, spikes.at[x], local.at[8])
    spike_own.start()

    start_sends = [
        remote(s0_ref.at[turn(x + d, NX)], start, s_send.at[d - 1], s_recv.at[0], fs=turn(x + d, NX)) for d in (1, 2, 3)
    ]

    @pl.when(is_composer & (x == seq_me))
    def _():
        for copy in start_sends:
            copy.start()
        pltpu.make_async_copy(s0_ref.at[x], start, s_recv.at[0]).start()

    spread(z)

    step = 64

    def norm(s):
        def some(i, _):
            r = pl.ds(pl.multiple_of(i * step, step), step)
            a = tok[s, 0, r, :].astype(F32)
            b = tok[s, 1, r, :].astype(F32)
            total = jnp.sum(a * a, axis=-1, keepdims=True) + jnp.sum(b * b, axis=-1, keepdims=True)
            scale = lax.rsqrt(total * (1.0 / (2 * features)) + EPS)
            at = pl.ds(pl.multiple_of(s * rows + i * step, step), step)
            normed[at, :features] = (a * scale * gain_ref[:, :features]).astype(BF16)
            normed[at, features:] = (b * scale * gain_ref[:, features:]).astype(BF16)
            return 0

        lax.fori_loop(0, rows // step, some, 0)

    def pass_on(i, src):
        remote(tok.at[src, c], tok.at[src, c], c_send.at[i], c_recv.at[i], tp=other).start()

    def tokens_near():
        for i in range(2):
            arrived(tok.at[left, c, halves[i]], t_recv.at[0, i])
            arrived(tok.at[right, c, halves[i]], t_recv.at[1, i])
        a, b = tok.at[left, c, halves[0]], tok.at[right, c, halves[1]]
        remote(a, a, t_send.at[2, 0], t_recv.at[2, 0], fs=right).start()
        remote(b, b, t_send.at[2, 1], t_recv.at[2, 1], fs=left).start()
        pass_on(1, left)
        pass_on(2, right)

    def norm_own():
        copies[7].wait()
        arrived(tok.at[x, other], c_recv.at[0])
        norm(x)

    def norm_near(i, src):
        arrived(tok.at[src, other], c_recv.at[i])
        norm(src)

    def tokens_far():
        for i in range(2):
            arrived(tok.at[over, c, halves[i]], t_recv.at[2, i])
        pass_on(3, over)

    hooks = (
        (2, norm_own),
        (4, tokens_near),
        (5, lambda: norm_near(1, left)),
        (6, lambda: norm_near(2, right)),
        (6, tokens_far),
    )

    for t in range(1, half):
        both_ways = ((0, turn(z - t, nz)), (1, turn(z + t, nz)))
        for pos in range(count):
            for way, src in both_ways:
                arrived(wbuf.at[src, chunks[pos]], ring_recv.at[way, t - 1, pos])
                if t < half - 1 or pos % 2 == way:
                    hop(t, pos, way, src).start()
        for i in range(len(shared)):
            for way, src in both_ways:
                to_partner(src, i).start()
        if t >= 2:
            for src in (turn(z - t + 1, nz), turn(z + t - 1, nz)):
                whole_piece(src)
                spread(src)
        for when, task in hooks:
            if t == min(when, half - 1):
                task()
    far = turn(z + half, nz)
    for pos in range(count):
        arrived(wbuf.at[far, chunks[pos]], ring_recv.at[pos % 2, half - 1, pos])
    for i in range(len(shared)):
        to_partner(far, i).start()
    norm_near(3, over)
    for src in (turn(z - half + 1, nz), turn(z + half - 1, nz)):
        whole_piece(src)
        spread(src)

    for d in (1, 2, 3):
        arrived(spikes.at[turn(x - d, NX)], k_recv.at[d - 1])
    spike_own.wait()

    def matrix(*js):
        return jnp.concatenate([wbuf[:, j].reshape(nz * HEAD, HEAD) for j in js], axis=1)

    def rows_of(s):
        return pl.ds(pl.multiple_of(s * rows, rows), rows)

    small = jnp.concatenate([decay_ref[...], strength_ref[...]], axis=0)
    for s in range(NX):
        gates[s] = dot_t(small, normed[s * rows : (s + 1) * rows, :])
    rate = jnp.exp(jnp.full((1, rows), rate_ref[head], F32))
    bias = bias_ref[head]
    edge = rows // 2
    row_half = lax.broadcasted_iota(jnp.int32, (edge, edge), 0)
    col_half = lax.broadcasted_iota(jnp.int32, (edge, edge), 1)

    def rounded(a):
        return a.astype(BF16).astype(F32)

    def terms(s):
        raw = rounded(jnp.dot(normed[rows_of(s), :], matrix(0, 1), preferred_element_type=F32))
        keys = unit_rows(silu(raw[:, :HEAD]))
        values = silu(raw[:, HEAD:])
        logit = rounded(gates[s, pl.ds(head, 1), :])
        beta = to_column(jax.nn.sigmoid(rounded(gates[s, pl.ds(HEADS + head, 1), :]) + bias))
        soft = jnp.maximum(logit, 0.0) + jnp.log1p(jnp.exp(-jnp.abs(logit)))
        log_row = spikes[s, pl.ds(x, 1), :] - rate * soft
        cum_col = jnp.sum(jnp.where(col <= row, log_row, 0.0), axis=1, keepdims=True)
        cum_row = to_row(cum_col)
        gamma = jnp.where(col <= row, jnp.exp(jnp.minimum(cum_col - cum_row, 0.0)), 0.0)
        grown = jnp.exp(cum_col)
        a_matrix = jnp.where(col < row, beta * dot_t(keys, keys) * gamma, 0.0)
        right = jnp.concatenate([beta * values, (beta * grown) * keys], axis=1).astype(BF16)
        total = cum_col[rows - 1 :, :]
        decayed = (keys * jnp.exp(total - cum_col)).astype(BF16)
        keys_at[s] = keys.astype(BF16)
        gammas[s] = gamma
        growth[s] = jnp.broadcast_to(grown, (rows, HEAD))
        return a_matrix, right, decayed, total

    def finish(group_of, all_terms):
        blocks = []
        for a_matrix, _, _, _ in all_terms:
            blocks += [a_matrix[:edge, :edge], a_matrix[edge:, edge:]]
        inverses = unit_lower_inverses(blocks, row_half, col_half)
        for n, s in enumerate(group_of):
            a_matrix, right, decayed, total = all_terms[n]
            first, second_half = inverses[2 * n], inverses[2 * n + 1]
            top = dot(first, right[:edge])
            low = dot(second_half, right[edge:].astype(F32) - dot(a_matrix[edge:, :edge], top))
            both = jnp.concatenate([top, low], axis=0).astype(BF16)
            solved[s] = both
            keep = jnp.exp(total)
            keep_hi = rounded(keep)
            tail = lax.broadcasted_iota(jnp.int32, (16, 2 * HEAD), 0)
            map_out[s, 0:HEAD, :] = dot_of_t(decayed, both).astype(BF16)
            map_out[s, HEAD:, :] = jnp.where(tail < 8, keep_hi, keep - keep_hi).astype(BF16)

    def send_map(s):
        owner = s * quarter + quarter // 2

        @pl.when((z != owner) & (z != last))
        def _():
            remote(map_out.at[s], map_in.at[z], map_send.at[s], map_recv.at[z], sp=owner).start()

        @pl.when((z == owner) & (z != last))
        def _():
            pltpu.make_async_copy(map_out.at[s], map_in.at[z], map_recv.at[z]).start()

    here = lax.div(z, quarter)
    far_pair = [lax.rem(here + k, NX) for k in (2, 1)]
    near_pair = [lax.rem(here + k, NX) for k in (3, 0)]
    finish(far_pair, [terms(s) for s in far_pair])
    whole_piece(far)
    spread(far)
    pending = [terms(s) for s in near_pair]
    for s in far_pair:
        send_map(s)
    finish(near_pair, pending)
    if paired:

        def shared_in(d, _):
            src = turn(z + d, nz)
            arrived(wbuf.at[src, 4 - parity], y_recv.at[src, 0])
            return 0

        lax.fori_loop(1, nz, shared_in, 0)
    for s in near_pair:
        send_map(s)

    def second(zz, _):
        for rel, core in ((0, c), (1, other)):
            first, again = wout.at[core * NX + left, zz], wout.at[core * NX + right, zz]
            arrived(first, near_recv.at[0, rel, zz])
            remote(first.at[0], first.at[0], far_send.at[0, rel, zz], far_recv.at[0, rel, zz], fs=right).start()
            arrived(again, near_recv.at[1, rel, zz])
            remote(again.at[1], again.at[1], far_send.at[1, rel, zz], far_recv.at[1, rel, zz], fs=left).start()
        return 0

    lax.fori_loop(0, half, second, 0)

    def gated(s):
        at = pl.ds(s * rows, rows)
        raw = rounded(jnp.dot(normed[at, :], matrix(3, 4), preferred_element_type=F32))
        glu = (raw[:, :HEAD] * jax.nn.sigmoid(raw[:, HEAD:])).astype(BF16)
        extended[s, pl.ds(PAD, rows), :] = glu.astype(F32)
        rim_out[s] = glu[rows - PAD :]

    def reads(s):
        at = pl.ds(s * rows, rows)
        raw = rounded(jnp.dot(normed[at, :], matrix(2), preferred_element_type=F32))
        query = unit_rows(silu(raw)) * HEAD ** (-0.5)
        scores = dot_t(query, keys_at[s]) * gammas[s]
        read = dot(scores, solved[s])
        base[s] = read[:, :HEAD]
        reader[s] = (growth[s] * query - read[:, HEAD:]).astype(BF16)

    for s in range(NX):
        gated(s)
    reads(0)

    @pl.when(z < last)
    def _():
        remote(rim_out, rim_in, rim_sem.at[0], rim_sem.at[1], sp=z + 1).start()

    for s in range(1, NX):
        reads(s)

    @pl.when(z > 0)
    def _():
        arrived(rim_in, rim_sem.at[1])
        extended[:, 0:PAD, :] = rim_in[...].astype(F32)

    @pl.when(z == 0)
    def _():
        extended[:, 0:PAD, :] = jnp.zeros((NX, PAD, HEAD), F32)

    piece = 64
    taps = taps_ref[:, lanes(head)]
    for s in range(NX):
        for r in range(rows // piece):
            conv = jnp.zeros((piece, HEAD), F32)
            for tap in range(KSIZE):
                conv = conv + taps[tap : tap + 1] * extended[s, pl.ds(r * piece + tap + PAD - KSIZE + 1, piece), :]
            conv_out[s, pl.ds(r * piece, piece), :] = conv.astype(BF16)

    def give(i):
        @pl.when(i != z)
        def _():
            remote(states.at[i], state_in.at[seq_me], state_send.at[i], state_recv.at[seq_me], sp=i).start()

        @pl.when(i == z)
        def _():
            pltpu.make_async_copy(states.at[i], state_in.at[seq_me], state_recv.at[seq_me]).start()

    @pl.when(is_composer)
    def _():
        arrived(start, s_recv.at[0])

        def advance(i, state):
            states[i] = state.astype(BF16)
            arrived(map_in.at[i], map_recv.at[i])
            block = map_in[i]
            keep = block[HEAD : HEAD + 1, :HEAD].astype(F32) + block[HEAD + 8 : HEAD + 9, :HEAD].astype(F32)
            high = state.astype(BF16)
            low = state - high.astype(F32)
            reduce = dot(block[:HEAD, HEAD:], high) + dot(block[:HEAD, HEAD:], low)
            result = keep * state - reduce + block[:HEAD, :HEAD].astype(F32)
            give(i)
            return result

        states[last] = lax.fori_loop(0, last, advance, start[...]).astype(BF16)

    def exchange(src, dst, send, recv):
        for d in range(NX):
            s = turn(x + d, NX)
            if d == 0:
                pltpu.make_async_copy(src.at[s], dst.at[:, lanes(head)], recv.at[0]).start()
            else:
                remote(src.at[s], dst.at[:, lanes(head)], send.at[d], recv.at[d], fs=s).start()
            remote(src.at[s], dst.at[:, lanes(head)], send.at[NX + d], recv.at[NX + d], fs=s, tp=other).start()

    def exchanged(src, dst, send, recv):
        for d in range(NX):
            source = turn(x - d, NX)
            arrived(dst.at[:, lanes(c * NX + source)], recv.at[d])
            arrived(dst.at[:, lanes(other * NX + source)], recv.at[NX + d])
            if d:
                remote(src.at[0], dst.at[:, lanes(head)], send.at[d], recv.at[d], fs=right).wait_send()
            remote(src.at[0], dst.at[:, lanes(head)], send.at[NX + d], recv.at[NX + d], fs=right).wait_send()

    exchange(conv_out, conv_all, conv_send, conv_recv)
    pl.when(is_composer)(lambda: give(last))

    head_gain = head_gain_ref[...]
    target = attn_all.at[:, lanes(head)]

    def send_attn(s):
        d = turn(s - x, NX)

        @pl.when(d == 0)
        def _():
            pltpu.make_async_copy(attn_out.at[s], target, attn_recv.at[0]).start()

        @pl.when(d != 0)
        def _():
            remote(attn_out.at[s], target, attn_send.at[d], attn_recv.at[d], fs=s).start()

        remote(attn_out.at[s], target, attn_send.at[NX + d], attn_recv.at[NX + d], fs=s, tp=other).start()

    order = [lax.rem(here + k, NX) for k in (0, 1, 3, 2)]
    for n, s in enumerate(order):
        arrived(state_in.at[s], state_recv.at[s])
        attn = base[s] + jnp.dot(reader[s], state_in[s], preferred_element_type=F32)
        scale = lax.rsqrt(jnp.mean(attn * attn, axis=-1, keepdims=True) + EPS)
        attn_out[s] = (attn * scale * head_gain).astype(BF16)
        if n:
            send_attn(order[n - 1])
    send_attn(order[-1])
    exchanged(conv_out, conv_all, conv_send, conv_recv)

    def channel_norm(i, _):
        at = pl.ds(pl.multiple_of(i * 64, 64), 64)
        conv = conv_all[at, :].astype(F32)
        mean = jnp.mean(conv, axis=-1, keepdims=True)
        var = jnp.mean(conv * conv, axis=-1, keepdims=True) - mean * mean
        conv_all[at, :] = silu((conv - mean) * lax.rsqrt(var + EPS) * channel_gain_ref[...]).astype(BF16)
        return 0

    lax.fori_loop(0, rows // 64, channel_norm, 0)

    def weights_in(zz, _):
        arrived(wout.at[head, zz], own_recv.at[0, zz])
        arrived(wout.at[other * NX + x, zz], own_recv.at[1, zz])
        for rel, core in ((0, c), (1, other)):
            for kind in range(2):
                arrived(wout.at[core * NX + over, zz, kind], far_recv.at[kind, rel, zz])
        return 0

    lax.fori_loop(0, half, weights_in, 0)

    def weights(j, kind):
        pair = [wout[:, 2 * j + i, kind].reshape(HEADS * HEAD, HEAD) for i in range(2)]
        return jnp.concatenate(pair, axis=1)

    def conv_part(j, _):
        partial[j] = jnp.dot(conv_all[...], weights(j, 1), preferred_element_type=F32)
        return 0

    lax.fori_loop(0, half // 2, conv_part, 0)
    exchanged(attn_out, attn_all, attn_send, attn_recv)

    def attn_part(j, _):
        total = partial[j] + jnp.dot(attn_all[...], weights(j, 0), preferred_element_type=F32)
        out_ref[:, pl.ds(pl.multiple_of(j * 2 * HEAD, 2 * HEAD), 2 * HEAD)] = total.astype(BF16)
        return 0

    lax.fori_loop(0, half // 2, attn_part, 0)

    def drain_ring(t, _):
        for pos in range(count):
            for way in range(2):
                hop(t, pos, way, z).wait_send()
        return 0

    lax.fori_loop(0, half - 1, drain_ring, 0)
    for pos in range(count):
        hop(half - 1, pos, pos % 2, z).wait_send()
    for i in range(2):
        for where, line in ((right, 0), (left, 1), (right, 2)):
            ref = tok.at[x, c, halves[i]]
            remote(ref, ref, t_send.at[line, i], t_recv.at[line, i], fs=where).wait_send()
    for i in range(4):
        remote(tok.at[x, c], tok.at[x, c], c_send.at[i], c_recv.at[i], tp=other).wait_send()
    for copy in spike_copies:
        copy.wait_send()

    @pl.when(is_composer & (x == seq_me))
    def _():
        for copy in start_sends:
            copy.wait_send()

    def drain(i, _):
        for way in range(2):
            remote(wbuf.at[i, pl.ds(5, 2)], wout.at[head, 0], near_send.at[way, i], near_recv.at[way, 0, 0], fs=right).wait_send()
        if paired:

            @pl.when(i != z)
            def _():
                to_partner(i, 0).wait_send()
                to_partner(i, 1).wait_send()

        @pl.when(is_composer & (i != z))
        def _():
            remote(states.at[i], state_in.at[seq_me], state_send.at[i], state_recv.at[seq_me], sp=i).wait_send()

        return 0

    lax.fori_loop(0, nz, drain, 0)

    def drain_half(zz, _):
        remote(wbuf.at[0, pl.ds(5, 2)], wout.at[head, zz], own_send.at[zz], own_recv.at[1, zz], tp=other).wait_send()
        for way in range(2):
            for rel in range(2):
                ref = wout.at[head, zz, 0]
                remote(ref, ref, far_send.at[way, rel, zz], far_recv.at[way, rel, zz], fs=right).wait_send()
        return 0

    lax.fori_loop(0, half, drain_half, 0)
    for s in range(NX):

        @pl.when((z != s * quarter + quarter // 2) & (z != last))
        def _(s=s):
            remote(map_out.at[s], map_in.at[z], map_send.at[s], map_recv.at[z], sp=0).wait_send()

    @pl.when(z < last)
    def _():
        remote(rim_out, rim_in, rim_sem.at[0], rim_sem.at[1], sp=z + 1).wait_send()


def mixed_tokens(nz, paired, tokens, *rest):
    rows, features = tokens.shape
    half = nz // 2
    count = 5 if paired else 7
    vmem = pl.BlockSpec(memory_space=pltpu.VMEM)
    smem = pl.BlockSpec(memory_space=pltpu.SMEM)
    dma = pltpu.SemaphoreType.DMA
    width = HEADS * HEAD
    return pl.pallas_call(
        functools.partial(kernel, nz, paired),
        name="mix",
        out_shape=jax.ShapeDtypeStruct((rows, half * HEAD), BF16),
        in_specs=[vmem] * 13 + [smem] * 2 + [vmem] * 3,
        out_specs=vmem,
        scratch_shapes=[
            pltpu.VMEM((NX, 2, rows, features), BF16),
            pltpu.VMEM((NX * rows, 2 * features), BF16),
            pltpu.VMEM((nz, 7, HEAD, HEAD), BF16),
            pltpu.VMEM((HEADS, half, 2, HEAD, HEAD), BF16),
            pltpu.VMEM((NX, 2 * HEADS, rows), F32),
            pltpu.VMEM((NX, NX, rows), F32),
            pltpu.VMEM((HEAD, HEAD), F32),
            pltpu.VMEM((NX, rows, HEAD), BF16),
            pltpu.VMEM((NX, rows, rows), F32),
            pltpu.VMEM((NX, rows, HEAD), F32),
            pltpu.VMEM((NX, rows, 2 * HEAD), BF16),
            pltpu.VMEM((NX, rows, HEAD), F32),
            pltpu.VMEM((NX, rows, HEAD), BF16),
            pltpu.VMEM((NX, HEAD + 16, 2 * HEAD), BF16),
            pltpu.VMEM((nz, HEAD + 16, 2 * HEAD), BF16),
            pltpu.VMEM((nz, HEAD, HEAD), BF16),
            pltpu.VMEM((NX, HEAD, HEAD), BF16),
            pltpu.VMEM((NX, PAD, HEAD), BF16),
            pltpu.VMEM((NX, PAD, HEAD), BF16),
            pltpu.VMEM((NX, PAD + rows, HEAD), F32),
            pltpu.VMEM((NX, rows, HEAD), BF16),
            pltpu.VMEM((rows, width), BF16),
            pltpu.VMEM((NX, rows, HEAD), BF16),
            pltpu.VMEM((rows, width), BF16),
            pltpu.VMEM((half // 2, rows, 2 * HEAD), F32),
            dma((2, half, count)),
            dma((2, half, count)),
            dma((nz, 2)),
            dma((nz, 2)),
            dma((2, nz)),
            dma((2, 2, half)),
            dma((2, 2, half)),
            dma((2, 2, half)),
            dma((half,)),
            dma((2, half)),
            dma((3, 2)),
            dma((3, 2)),
            dma((4,)),
            dma((4,)),
            dma((3,)),
            dma((3,)),
            dma((3,)),
            dma((1,)),
            dma((9,)),
            dma((NX,)),
            dma((nz,)),
            dma((nz,)),
            dma((NX,)),
            dma((2,)),
            dma((2 * NX,)),
            dma((2 * NX,)),
            dma((2 * NX,)),
            dma((2 * NX,)),
        ],
        compiler_params=pltpu.CompilerParams(
            collective_id=0, has_side_effects=True, vmem_limit_bytes=60 * 1024 * 1024
        ),
    )(tokens, *rest)


def on_device(
    nz,
    paired,
    tokens,
    input_norm_gain,
    query_weight,
    key_weight,
    value_weight,
    decay_gate_weight,
    write_strength_weight,
    up_weight,
    gate_half_weight,
    log_decay_rate,
    write_strength_bias,
    decay_spike_added,
    starting_state,
    head_norm_gain,
    convolution_kernel,
    channel_norm_gain,
    delta_output_rows,
    convolution_output_rows,
):
    mixed = mixed_tokens(
        nz,
        paired,
        tokens[0],
        key_weight,
        value_weight,
        query_weight,
        up_weight,
        gate_half_weight,
        delta_output_rows,
        convolution_output_rows,
        input_norm_gain[None],
        decay_gate_weight.T,
        write_strength_weight.T,
        decay_spike_added[0].T,
        starting_state[0],
        log_decay_rate,
        write_strength_bias,
        head_norm_gain[None],
        convolution_kernel,
        channel_norm_gain[None],
    )
    return mixed[None]


def solution(mesh):
    return jax.shard_map(
        functools.partial(on_device, mesh.shape["sp"], mesh.shape["grp"] % 2 == 0),
        mesh=mesh,
        in_specs=(
            P(("grp", "fs"), "sp", "tp"),
            P(),
            P("sp", "tp"),
            P("sp", "tp"),
            P("sp", "tp"),
            P(),
            P(),
            P("sp", "tp"),
            P("sp", "tp"),
            P(),
            P(),
            P(("grp", "fs"), "sp", "tp"),
            P(("grp", "fs"), "tp", None, None),
            P(),
            P(),
            P(),
            P("tp", "sp"),
            P("tp", "sp"),
        ),
        out_specs=P(("grp", "fs"), "sp", "tp"),
        check_vma=False,
    )
```

```python
import functools

import jax
import jax.numpy as jnp
from jax import lax
from jax.experimental import pallas as pl
from jax.experimental.pallas import tpu as pltpu
from jax.sharding import PartitionSpec as P

HEADS = 8
HEAD = 128
KSIZE = 31
NX = 4
PAD = 32
EPS = 1e-06
MESH = pl.DeviceIdType.MESH
F32 = jnp.float32
BF16 = jnp.bfloat16


def remote(src, dst, send, recv, **where):
    return pltpu.make_async_remote_copy(
        src_ref=src, dst_ref=dst, send_sem=send, recv_sem=recv, device_id=where, device_id_type=MESH
    )


def arrived(ref, sem):
    pltpu.make_async_copy(ref, ref, sem).wait()


def turn(i, n):
    return lax.rem(i + n, n)


def lanes(i):
    return pl.ds(pl.multiple_of(i * HEAD, HEAD), HEAD)


def composer(z, c, nz):
    quarter = nz // NX
    return lax.div(z, quarter), lax.rem(z, quarter) == (1 - c) * (quarter // 2)


def dot(a, b):
    return jnp.dot(a.astype(BF16), b.astype(BF16), preferred_element_type=F32)


def dot_t(a, b):
    dims = (((1,), (1,)), ((), ()))
    return lax.dot_general(a.astype(BF16), b.astype(BF16), dims, preferred_element_type=F32)


def dot_of_t(a, b):
    dims = (((0,), (0,)), ((), ()))
    return lax.dot_general(a.astype(BF16), b.astype(BF16), dims, preferred_element_type=F32)


def silu(a):
    return a * jax.nn.sigmoid(a)


def unit_rows(a):
    return a * lax.rsqrt(jnp.sum(a * a, axis=-1, keepdims=True) + EPS)


def unit_lower_inverses(blocks, row, col):
    size = blocks[0].shape[0]
    eye = jnp.where(row == col, 1.0, 0.0)
    below = (row - col == 1) & (lax.rem(row, 2) == 1)
    inverses = [eye - jnp.where(below, a, 0.0) for a in blocks]
    width = 2
    while width < size:
        same = lax.div(row, 2 * width) == lax.div(col, 2 * width)
        mask = same & (lax.div(row, width) != lax.div(col, width))
        steps = [dot(b, jnp.where(mask, a, 0.0)) for a, b in zip(blocks, inverses)]
        inverses = [b - dot(p, b) for p, b in zip(steps, inverses)]
        width *= 2
    return inverses


def kernel(
    nz,
    paired,
    tok_ref,
    k_ref,
    v_ref,
    q_ref,
    up_ref,
    gate_ref,
    do_ref,
    co_ref,
    gain_ref,
    decay_ref,
    strength_ref,
    spike_ref,
    s0_ref,
    rate_ref,
    bias_ref,
    head_gain_ref,
    taps_ref,
    channel_gain_ref,
    out_ref,
    tok,
    normed,
    wbuf,
    wout,
    gates,
    spikes,
    start,
    keys_at,
    gammas,
    growth,
    solved,
    base,
    reader,
    map_out,
    map_in,
    states,
    state_in,
    rim_out,
    rim_in,
    extended,
    conv_out,
    conv_all,
    attn_out,
    attn_all,
    partial,
    ring_send,
    ring_recv,
    y_send,
    y_recv,
    near_send,
    near_recv,
    far_send,
    far_recv,
    own_send,
    own_recv,
    t_send,
    t_recv,
    c_send,
    c_recv,
    k_send,
    k_recv,
    s_send,
    s_recv,
    local,
    map_send,
    map_recv,
    state_send,
    state_recv,
    rim_sem,
    conv_send,
    conv_recv,
    attn_send,
    attn_recv,
):
    z, x, c = lax.axis_index("sp"), lax.axis_index("fs"), lax.axis_index("tp")
    up, down = turn(z + 1, nz), turn(z - 1, nz)
    right, left, over = turn(x + 1, NX), turn(x - 1, NX), turn(x + 2, NX)
    other = 1 - c
    head = c * NX + x
    half = nz // 2
    quarter = nz // NX
    last = nz - 1
    rows, features = tok_ref.shape
    seq_me, is_composer = composer(z, c, nz)
    group = lax.axis_index("grp")
    parity = lax.rem(group, 2)
    partner = group + 1 - 2 * parity

    neighbours = [{"sp": up}, {"sp": down}, {"fs": right}, {"fs": left}, {"fs": over}, {"tp": other}]
    neighbours += [{"fs": right, "tp": other}, {"fs": left, "tp": other}, {"fs": over, "tp": other}]
    if paired:
        neighbours.append({"grp": partner})
    barrier = pltpu.get_barrier_semaphore()
    for where in neighbours:
        pl.semaphore_signal(barrier, inc=1, device_id=where, device_id_type=MESH)

    own = [w.at[:, lanes(x)] for w in (k_ref, v_ref, q_ref, up_ref, gate_ref)]
    own += [w.at[lanes(x), :] for w in (do_ref, co_ref)]
    copies = [pltpu.make_async_copy(a, wbuf.at[z, j], local.at[j]) for j, a in enumerate(own)]
    copies.append(pltpu.make_async_copy(tok_ref, tok.at[x, c], local.at[7]))
    for copy in copies:
        copy.start()

    row = lax.broadcasted_iota(jnp.int32, (rows, rows), 0)
    col = lax.broadcasted_iota(jnp.int32, (rows, rows), 1)

    def to_row(column):
        return jnp.sum(jnp.where(row == col, column, 0.0), axis=0, keepdims=True)

    def to_column(line):
        return jnp.sum(jnp.where(row == col, line, 0.0), axis=1, keepdims=True)

    if paired:
        chunks, shared = [0, 1, 2, 3 + parity, 5 + parity], (3, 4)
    else:
        chunks, shared = list(range(7)), ()
    count = len(chunks)

    def hop(t, pos, way, src):
        ref = wbuf.at[src, chunks[pos]]
        return remote(ref, ref, ring_send.at[way, t, pos], ring_recv.at[way, t, pos], sp=up if way == 0 else down)

    def to_partner(src, i):
        ref = wbuf.at[src, chunks[shared[i]]]
        return remote(ref, ref, y_send.at[src, i], y_recv.at[src, i], grp=partner)

    def whole_piece(src):
        if paired:
            arrived(wbuf.at[src, 6 - parity], y_recv.at[src, 1])

    def spread(src):
        core, zz = lax.div(src, half), lax.rem(src, half)
        other_core = core + c - 2 * core * c
        piece, target = wbuf.at[src, pl.ds(5, 2)], wout.at[head, zz]
        remote(piece, target, near_send.at[0, src], near_recv.at[0, other_core, zz], fs=right, tp=core).start()
        remote(piece, target, near_send.at[1, src], near_recv.at[1, other_core, zz], fs=left, tp=core).start()

        @pl.when(other_core == 0)
        def _():
            pltpu.make_async_copy(piece, target, own_recv.at[0, zz]).start()

        @pl.when(other_core == 1)
        def _():
            remote(piece, target, own_send.at[zz], own_recv.at[1, zz], tp=other).start()

    pl.semaphore_wait(barrier, len(neighbours))
    for j in range(7):
        copies[j].wait()
    for pos in range(count):
        hop(0, pos, 0, z).start()
        hop(0, pos, 1, z).start()

    part = rows // 2
    halves = (pl.ds(0, part), pl.ds(part, part))
    for i in range(2):
        src = tok_ref.at[halves[i]]
        dst = tok.at[x, c, halves[i]]
        remote(src, dst, t_send.at[0, i], t_recv.at[0, i], fs=right).start()
        remote(src, dst, t_send.at[1, i], t_recv.at[1, i], fs=left).start()
    remote(tok_ref, tok.at[x, c], c_send.at[0], c_recv.at[0], tp=other).start()
    spike_copies = [
        remote(spike_ref, spikes.at[x], k_send.at[d - 1], k_recv.at[d - 1], fs=turn(x + d, NX)) for d in (1, 2, 3)
    ]
    for copy in spike_copies:
        copy.start()
    spike_own = pltpu.make_async_copy(spike_ref, spikes.at[x], local.at[8])
    spike_own.start()

    start_sends = [
        remote(s0_ref.at[turn(x + d, NX)], start, s_send.at[d - 1], s_recv.at[0], fs=turn(x + d, NX)) for d in (1, 2, 3)
    ]

    @pl.when(is_composer & (x == seq_me))
    def _():
        for copy in start_sends:
            copy.start()
        pltpu.make_async_copy(s0_ref.at[x], start, s_recv.at[0]).start()

    spread(z)

    step = 64

    def norm(s):
        def some(i, _):
            r = pl.ds(pl.multiple_of(i * step, step), step)
            a = tok[s, 0, r, :].astype(F32)
            b = tok[s, 1, r, :].astype(F32)
            total = jnp.sum(a * a, axis=-1, keepdims=True) + jnp.sum(b * b, axis=-1, keepdims=True)
            scale = lax.rsqrt(total * (1.0 / (2 * features)) + EPS)
            at = pl.ds(pl.multiple_of(s * rows + i * step, step), step)
            normed[at, :features] = (a * scale * gain_ref[:, :features]).astype(BF16)
            normed[at, features:] = (b * scale * gain_ref[:, features:]).astype(BF16)
            return 0

        lax.fori_loop(0, rows // step, some, 0)

    def pass_on(i, src):
        remote(tok.at[src, c], tok.at[src, c], c_send.at[i], c_recv.at[i], tp=other).start()

    def tokens_near():
        for i in range(2):
            arrived(tok.at[left, c, halves[i]], t_recv.at[0, i])
            arrived(tok.at[right, c, halves[i]], t_recv.at[1, i])
        a, b = tok.at[left, c, halves[0]], tok.at[right, c, halves[1]]
        remote(a, a, t_send.at[2, 0], t_recv.at[2, 0], fs=right).start()
        remote(b, b, t_send.at[2, 1], t_recv.at[2, 1], fs=left).start()
        pass_on(1, left)
        pass_on(2, right)

    def norm_own():
        copies[7].wait()
        arrived(tok.at[x, other], c_recv.at[0])
        norm(x)

    def norm_near(i, src):
        arrived(tok.at[src, other], c_recv.at[i])
        norm(src)

    def tokens_far():
        for i in range(2):
            arrived(tok.at[over, c, halves[i]], t_recv.at[2, i])
        pass_on(3, over)

    hooks = (
        (2, norm_own),
        (4, tokens_near),
        (5, lambda: norm_near(1, left)),
        (6, lambda: norm_near(2, right)),
        (6, tokens_far),
    )

    for t in range(1, half):
        both_ways = ((0, turn(z - t, nz)), (1, turn(z + t, nz)))
        for pos in range(count):
            for way, src in both_ways:
                arrived(wbuf.at[src, chunks[pos]], ring_recv.at[way, t - 1, pos])
                if t < half - 1 or pos % 2 == way:
                    hop(t, pos, way, src).start()
        for i in range(len(shared)):
            for way, src in both_ways:
                to_partner(src, i).start()
        if t >= 2:
            for src in (turn(z - t + 1, nz), turn(z + t - 1, nz)):
                whole_piece(src)
                spread(src)
        for when, task in hooks:
            if t == min(when, half - 1):
                task()
    norm_near(3, over)
    for src in (turn(z - half + 1, nz), turn(z + half - 1, nz)):
        whole_piece(src)
        spread(src)
    far = turn(z + half, nz)

    def last_hop(positions):
        for pos in positions:
            arrived(wbuf.at[far, chunks[pos]], ring_recv.at[pos % 2, half - 1, pos])

    last_hop(range(2))

    for d in (1, 2, 3):
        arrived(spikes.at[turn(x - d, NX)], k_recv.at[d - 1])
    spike_own.wait()

    def matrix(*js):
        return jnp.concatenate([wbuf[:, j].reshape(nz * HEAD, HEAD) for j in js], axis=1)

    def rows_of(s):
        return pl.ds(pl.multiple_of(s * rows, rows), rows)

    small = jnp.concatenate([decay_ref[...], strength_ref[...]], axis=0)
    for s in range(NX):
        gates[s] = dot_t(small, normed[s * rows : (s + 1) * rows, :])
    rate = jnp.exp(jnp.full((1, rows), rate_ref[head], F32))
    bias = bias_ref[head]
    edge = rows // 2
    row_half = lax.broadcasted_iota(jnp.int32, (edge, edge), 0)
    col_half = lax.broadcasted_iota(jnp.int32, (edge, edge), 1)

    def rounded(a):
        return a.astype(BF16).astype(F32)

    def terms(s):
        raw = rounded(jnp.dot(normed[rows_of(s), :], matrix(0, 1), preferred_element_type=F32))
        keys = unit_rows(silu(raw[:, :HEAD]))
        values = silu(raw[:, HEAD:])
        logit = rounded(gates[s, pl.ds(head, 1), :])
        beta = to_column(jax.nn.sigmoid(rounded(gates[s, pl.ds(HEADS + head, 1), :]) + bias))
        soft = jnp.maximum(logit, 0.0) + jnp.log1p(jnp.exp(-jnp.abs(logit)))
        log_row = spikes[s, pl.ds(x, 1), :] - rate * soft
        cum_col = jnp.sum(jnp.where(col <= row, log_row, 0.0), axis=1, keepdims=True)
        cum_row = to_row(cum_col)
        gamma = jnp.where(col <= row, jnp.exp(jnp.minimum(cum_col - cum_row, 0.0)), 0.0)
        grown = jnp.exp(cum_col)
        a_matrix = jnp.where(col < row, beta * dot_t(keys, keys) * gamma, 0.0)
        right = jnp.concatenate([beta * values, (beta * grown) * keys], axis=1).astype(BF16)
        total = cum_col[rows - 1 :, :]
        decayed = (keys * jnp.exp(total - cum_col)).astype(BF16)
        keys_at[s] = keys.astype(BF16)
        gammas[s] = gamma
        growth[s] = jnp.broadcast_to(grown, (rows, HEAD))
        return a_matrix, right, decayed, total

    def finish(group_of, all_terms):
        blocks = []
        for a_matrix, _, _, _ in all_terms:
            blocks += [a_matrix[:edge, :edge], a_matrix[edge:, edge:]]
        inverses = unit_lower_inverses(blocks, row_half, col_half)
        for n, s in enumerate(group_of):
            a_matrix, right, decayed, total = all_terms[n]
            first, second_half = inverses[2 * n], inverses[2 * n + 1]
            top = dot(first, right[:edge])
            low = dot(second_half, right[edge:].astype(F32) - dot(a_matrix[edge:, :edge], top))
            both = jnp.concatenate([top, low], axis=0).astype(BF16)
            solved[s] = both
            keep = jnp.exp(total)
            keep_hi = rounded(keep)
            tail = lax.broadcasted_iota(jnp.int32, (8, 2 * HEAD), 0)
            map_out[s, 0:HEAD, :] = dot_of_t(decayed, both).astype(BF16)
            map_out[s, HEAD:, :] = jnp.where(tail < 4, keep_hi, keep - keep_hi).astype(BF16)

    def send_map(s):
        owner = s * quarter + other * (quarter // 2)

        @pl.when((z != owner) & (z != last))
        def _():
            remote(map_out.at[s], map_in.at[z], map_send.at[s], map_recv.at[z], sp=owner).start()

        @pl.when((z == owner) & (z != last))
        def _():
            pltpu.make_async_copy(map_out.at[s], map_in.at[z], map_recv.at[z]).start()

    def reads(s):
        at = rows_of(s)
        raw = rounded(jnp.dot(normed[at, :], matrix(2), preferred_element_type=F32))
        query = unit_rows(silu(raw)) * HEAD ** (-0.5)
        scores = dot_t(query, keys_at[s]) * gammas[s]
        read = dot(scores, solved[s])
        base[s] = read[:, :HEAD]
        reader[s] = (growth[s] * query - read[:, HEAD:]).astype(BF16)

    here = lax.div(z, quarter)
    far_pair = [lax.rem(here + k, NX) for k in (2, 1)]
    near_pair = [lax.rem(here + k, NX) for k in (3, 0)]
    finish(far_pair, [terms(s) for s in far_pair])
    last_hop(range(2, count))
    for i in range(len(shared)):
        to_partner(far, i).start()
    pending = [terms(s) for s in near_pair]
    for s in far_pair:
        send_map(s)
    finish(near_pair, pending)
    reads(far_pair[0])
    for s in near_pair:
        send_map(s)
    whole_piece(far)
    spread(far)
    if paired:

        def shared_in(d, _):
            src = turn(z + d, nz)
            arrived(wbuf.at[src, 4 - parity], y_recv.at[src, 0])
            return 0

        lax.fori_loop(1, nz, shared_in, 0)

    def second(zz, _):
        for rel, core in ((0, c), (1, other)):
            first, again = wout.at[core * NX + left, zz], wout.at[core * NX + right, zz]
            arrived(first, near_recv.at[0, rel, zz])
            remote(first.at[0], first.at[0], far_send.at[0, rel, zz], far_recv.at[0, rel, zz], fs=right).start()
            arrived(again, near_recv.at[1, rel, zz])
            remote(again.at[1], again.at[1], far_send.at[1, rel, zz], far_recv.at[1, rel, zz], fs=left).start()
        return 0

    lax.fori_loop(0, half, second, 0)

    def gated(s):
        at = pl.ds(s * rows, rows)
        raw = rounded(jnp.dot(normed[at, :], matrix(3, 4), preferred_element_type=F32))
        glu = (raw[:, :HEAD] * jax.nn.sigmoid(raw[:, HEAD:])).astype(BF16)
        extended[s, pl.ds(PAD, rows), :] = glu.astype(F32)
        rim_out[s] = glu[rows - PAD :]

    for s in range(NX):
        gated(s)
    reads(far_pair[1])

    @pl.when(z < last)
    def _():
        remote(rim_out, rim_in, rim_sem.at[0], rim_sem.at[1], sp=z + 1).start()

    for s in near_pair:
        reads(s)

    @pl.when(z > 0)
    def _():
        arrived(rim_in, rim_sem.at[1])
        extended[:, 0:PAD, :] = rim_in[...].astype(F32)

    @pl.when(z == 0)
    def _():
        extended[:, 0:PAD, :] = jnp.zeros((NX, PAD, HEAD), F32)

    piece = 64
    taps = taps_ref[:, lanes(head)]
    for s in range(NX):
        for r in range(rows // piece):
            conv = jnp.zeros((piece, HEAD), F32)
            for tap in range(KSIZE):
                conv = conv + taps[tap : tap + 1] * extended[s, pl.ds(r * piece + tap + PAD - KSIZE + 1, piece), :]
            conv_out[s, pl.ds(r * piece, piece), :] = conv.astype(BF16)

    def give(i):
        @pl.when(i != z)
        def _():
            remote(states.at[i], state_in.at[seq_me], state_send.at[i], state_recv.at[seq_me], sp=i).start()

        @pl.when(i == z)
        def _():
            pltpu.make_async_copy(states.at[i], state_in.at[seq_me], state_recv.at[seq_me]).start()

    @pl.when(is_composer)
    def _():
        arrived(start, s_recv.at[0])
        states[0] = start[...].astype(BF16)

        def advance(i, state):
            give(i)
            arrived(map_in.at[i], map_recv.at[i])
            block = map_in[i]
            keep = block[HEAD : HEAD + 1, :HEAD].astype(F32) + block[HEAD + 4 : HEAD + 5, :HEAD].astype(F32)
            high = state.astype(BF16)
            low = state - high.astype(F32)
            reduce = dot(block[:HEAD, HEAD:], high) + dot(block[:HEAD, HEAD:], low)
            result = keep * state - reduce + block[:HEAD, :HEAD].astype(F32)
            states[i + 1] = result.astype(BF16)
            return result

        lax.fori_loop(0, last, advance, start[...])

    def exchange(src, dst, send, recv):
        for d in range(NX):
            s = turn(x + d, NX)
            if d == 0:
                pltpu.make_async_copy(src.at[s], dst.at[:, lanes(head)], recv.at[0]).start()
            else:
                remote(src.at[s], dst.at[:, lanes(head)], send.at[d], recv.at[d], fs=s).start()
            remote(src.at[s], dst.at[:, lanes(head)], send.at[NX + d], recv.at[NX + d], fs=s, tp=other).start()

    def exchanged(src, dst, send, recv):
        for d in range(NX):
            source = turn(x - d, NX)
            arrived(dst.at[:, lanes(c * NX + source)], recv.at[d])
            arrived(dst.at[:, lanes(other * NX + source)], recv.at[NX + d])
            if d:
                remote(src.at[0], dst.at[:, lanes(head)], send.at[d], recv.at[d], fs=right).wait_send()
            remote(src.at[0], dst.at[:, lanes(head)], send.at[NX + d], recv.at[NX + d], fs=right).wait_send()

    exchange(conv_out, conv_all, conv_send, conv_recv)
    pl.when(is_composer)(lambda: give(last))

    head_gain = head_gain_ref[...]
    target = attn_all.at[:, lanes(head)]

    def send_attn(s):
        d = turn(s - x, NX)

        @pl.when(d == 0)
        def _():
            pltpu.make_async_copy(attn_out.at[s], target, attn_recv.at[0]).start()

        @pl.when(d != 0)
        def _():
            remote(attn_out.at[s], target, attn_send.at[d], attn_recv.at[d], fs=s).start()

        remote(attn_out.at[s], target, attn_send.at[NX + d], attn_recv.at[NX + d], fs=s, tp=other).start()

    order = [lax.rem(here + k, NX) for k in (0, 1, 3, 2)]
    for n, s in enumerate(order):
        arrived(state_in.at[s], state_recv.at[s])
        attn = base[s] + jnp.dot(reader[s], state_in[s], preferred_element_type=F32)
        scale = lax.rsqrt(jnp.mean(attn * attn, axis=-1, keepdims=True) + EPS)
        attn_out[s] = (attn * scale * head_gain).astype(BF16)
        if n:
            send_attn(order[n - 1])
    send_attn(order[-1])
    exchanged(conv_out, conv_all, conv_send, conv_recv)

    def channel_norm(i, _):
        at = pl.ds(pl.multiple_of(i * 64, 64), 64)
        conv = conv_all[at, :].astype(F32)
        mean = jnp.mean(conv, axis=-1, keepdims=True)
        var = jnp.mean(conv * conv, axis=-1, keepdims=True) - mean * mean
        conv_all[at, :] = silu((conv - mean) * lax.rsqrt(var + EPS) * channel_gain_ref[...]).astype(BF16)
        return 0

    lax.fori_loop(0, rows // 64, channel_norm, 0)

    def weights_in(zz, _):
        arrived(wout.at[head, zz], own_recv.at[0, zz])
        arrived(wout.at[other * NX + x, zz], own_recv.at[1, zz])
        for rel, core in ((0, c), (1, other)):
            for kind in range(2):
                arrived(wout.at[core * NX + over, zz, kind], far_recv.at[kind, rel, zz])
        return 0

    lax.fori_loop(0, half, weights_in, 0)

    def weights(j, kind):
        pair = [wout[:, 2 * j + i, kind].reshape(HEADS * HEAD, HEAD) for i in range(2)]
        return jnp.concatenate(pair, axis=1)

    def conv_part(j, _):
        partial[j] = jnp.dot(conv_all[...], weights(j, 1), preferred_element_type=F32)
        return 0

    lax.fori_loop(0, half // 2, conv_part, 0)
    def drain_ring(t, _):
        for pos in range(count):
            for way in range(2):
                hop(t, pos, way, z).wait_send()
        return 0

    lax.fori_loop(0, half - 1, drain_ring, 0)
    for pos in range(count):
        hop(half - 1, pos, pos % 2, z).wait_send()
    for i in range(2):
        for where, line in ((right, 0), (left, 1), (right, 2)):
            ref = tok.at[x, c, halves[i]]
            remote(ref, ref, t_send.at[line, i], t_recv.at[line, i], fs=where).wait_send()
    for i in range(4):
        remote(tok.at[x, c], tok.at[x, c], c_send.at[i], c_recv.at[i], tp=other).wait_send()
    for copy in spike_copies:
        copy.wait_send()

    @pl.when(is_composer & (x == seq_me))
    def _():
        for copy in start_sends:
            copy.wait_send()

    def drain(i, _):
        for way in range(2):
            remote(wbuf.at[i, pl.ds(5, 2)], wout.at[head, 0], near_send.at[way, i], near_recv.at[way, 0, 0], fs=right).wait_send()
        if paired:

            @pl.when(i != z)
            def _():
                to_partner(i, 0).wait_send()
                to_partner(i, 1).wait_send()

        @pl.when(is_composer & (i != z))
        def _():
            remote(states.at[i], state_in.at[seq_me], state_send.at[i], state_recv.at[seq_me], sp=i).wait_send()

        return 0

    lax.fori_loop(0, nz, drain, 0)

    def drain_half(zz, _):
        remote(wbuf.at[0, pl.ds(5, 2)], wout.at[head, zz], own_send.at[zz], own_recv.at[1, zz], tp=other).wait_send()
        for way in range(2):
            for rel in range(2):
                ref = wout.at[head, zz, 0]
                remote(ref, ref, far_send.at[way, rel, zz], far_recv.at[way, rel, zz], fs=right).wait_send()
        return 0

    lax.fori_loop(0, half, drain_half, 0)
    for s in range(NX):

        @pl.when((z != s * quarter + other * (quarter // 2)) & (z != last))
        def _(s=s):
            remote(map_out.at[s], map_in.at[z], map_send.at[s], map_recv.at[z], sp=0).wait_send()

    @pl.when(z < last)
    def _():
        remote(rim_out, rim_in, rim_sem.at[0], rim_sem.at[1], sp=z + 1).wait_send()

    exchanged(attn_out, attn_all, attn_send, attn_recv)

    def attn_part(j, _):
        total = partial[j] + jnp.dot(attn_all[...], weights(j, 0), preferred_element_type=F32)
        out_ref[:, pl.ds(pl.multiple_of(j * 2 * HEAD, 2 * HEAD), 2 * HEAD)] = total.astype(BF16)
        return 0

    lax.fori_loop(0, half // 2, attn_part, 0)


def mixed_tokens(nz, paired, tokens, *rest):
    rows, features = tokens.shape
    half = nz // 2
    count = 5 if paired else 7
    vmem = pl.BlockSpec(memory_space=pltpu.VMEM)
    smem = pl.BlockSpec(memory_space=pltpu.SMEM)
    dma = pltpu.SemaphoreType.DMA
    width = HEADS * HEAD
    return pl.pallas_call(
        functools.partial(kernel, nz, paired),
        name="mix",
        out_shape=jax.ShapeDtypeStruct((rows, half * HEAD), BF16),
        in_specs=[vmem] * 13 + [smem] * 2 + [vmem] * 3,
        out_specs=vmem,
        scratch_shapes=[
            pltpu.VMEM((NX, 2, rows, features), BF16),
            pltpu.VMEM((NX * rows, 2 * features), BF16),
            pltpu.VMEM((nz, 7, HEAD, HEAD), BF16),
            pltpu.VMEM((HEADS, half, 2, HEAD, HEAD), BF16),
            pltpu.VMEM((NX, 2 * HEADS, rows), F32),
            pltpu.VMEM((NX, NX, rows), F32),
            pltpu.VMEM((HEAD, HEAD), F32),
            pltpu.VMEM((NX, rows, HEAD), BF16),
            pltpu.VMEM((NX, rows, rows), F32),
            pltpu.VMEM((NX, rows, HEAD), F32),
            pltpu.VMEM((NX, rows, 2 * HEAD), BF16),
            pltpu.VMEM((NX, rows, HEAD), F32),
            pltpu.VMEM((NX, rows, HEAD), BF16),
            pltpu.VMEM((NX, HEAD + 8, 2 * HEAD), BF16),
            pltpu.VMEM((nz, HEAD + 8, 2 * HEAD), BF16),
            pltpu.VMEM((nz, HEAD, HEAD), BF16),
            pltpu.VMEM((NX, HEAD, HEAD), BF16),
            pltpu.VMEM((NX, PAD, HEAD), BF16),
            pltpu.VMEM((NX, PAD, HEAD), BF16),
            pltpu.VMEM((NX, PAD + rows, HEAD), F32),
            pltpu.VMEM((NX, rows, HEAD), BF16),
            pltpu.VMEM((rows, width), BF16),
            pltpu.VMEM((NX, rows, HEAD), BF16),
            pltpu.VMEM((rows, width), BF16),
            pltpu.VMEM((half // 2, rows, 2 * HEAD), F32),
            dma((2, half, count)),
            dma((2, half, count)),
            dma((nz, 2)),
            dma((nz, 2)),
            dma((2, nz)),
            dma((2, 2, half)),
            dma((2, 2, half)),
            dma((2, 2, half)),
            dma((half,)),
            dma((2, half)),
            dma((3, 2)),
            dma((3, 2)),
            dma((4,)),
            dma((4,)),
            dma((3,)),
            dma((3,)),
            dma((3,)),
            dma((1,)),
            dma((9,)),
            dma((NX,)),
            dma((nz,)),
            dma((nz,)),
            dma((NX,)),
            dma((2,)),
            dma((2 * NX,)),
            dma((2 * NX,)),
            dma((2 * NX,)),
            dma((2 * NX,)),
        ],
        compiler_params=pltpu.CompilerParams(
            collective_id=0, has_side_effects=True, vmem_limit_bytes=60 * 1024 * 1024
        ),
    )(tokens, *rest)


def on_device(
    nz,
    paired,
    tokens,
    input_norm_gain,
    query_weight,
    key_weight,
    value_weight,
    decay_gate_weight,
    write_strength_weight,
    up_weight,
    gate_half_weight,
    log_decay_rate,
    write_strength_bias,
    decay_spike_added,
    starting_state,
    head_norm_gain,
    convolution_kernel,
    channel_norm_gain,
    delta_output_rows,
    convolution_output_rows,
):
    mixed = mixed_tokens(
        nz,
        paired,
        tokens[0],
        key_weight,
        value_weight,
        query_weight,
        up_weight,
        gate_half_weight,
        delta_output_rows,
        convolution_output_rows,
        input_norm_gain[None],
        decay_gate_weight.T,
        write_strength_weight.T,
        decay_spike_added[0].T,
        starting_state[0],
        log_decay_rate,
        write_strength_bias,
        head_norm_gain[None],
        convolution_kernel,
        channel_norm_gain[None],
    )
    return mixed[None]


def solution(mesh):
    return jax.shard_map(
        functools.partial(on_device, mesh.shape["sp"], mesh.shape["grp"] % 2 == 0),
        mesh=mesh,
        in_specs=(
            P(("grp", "fs"), "sp", "tp"),
            P(),
            P("sp", "tp"),
            P("sp", "tp"),
            P("sp", "tp"),
            P(),
            P(),
            P("sp", "tp"),
            P("sp", "tp"),
            P(),
            P(),
            P(("grp", "fs"), "sp", "tp"),
            P(("grp", "fs"), "tp", None, None),
            P(),
            P(),
            P(),
            P("tp", "sp"),
            P("tp", "sp"),
        ),
        out_specs=P(("grp", "fs"), "sp", "tp"),
        check_vma=False,
    )
```

```python
import functools

import jax
import jax.numpy as jnp
from jax import lax
from jax.experimental import pallas as pl
from jax.experimental.pallas import tpu as pltpu
from jax.sharding import PartitionSpec as P

HEADS = 8
HEAD = 128
KSIZE = 31
NX = 4
PAD = 32
EPS = 1e-06
MESH = pl.DeviceIdType.MESH
F32 = jnp.float32
BF16 = jnp.bfloat16


def remote(src, dst, send, recv, **where):
    return pltpu.make_async_remote_copy(
        src_ref=src, dst_ref=dst, send_sem=send, recv_sem=recv, device_id=where, device_id_type=MESH
    )


def arrived(ref, sem):
    pltpu.make_async_copy(ref, ref, sem).wait()


def turn(i, n):
    return lax.rem(i + n, n)


def lanes(i):
    return pl.ds(pl.multiple_of(i * HEAD, HEAD), HEAD)


def composer(z, c, nz):
    quarter = nz // NX
    return lax.div(z, quarter), lax.rem(z, quarter) == (1 - c) * (quarter // 2)


def dot(a, b):
    return jnp.dot(a.astype(BF16), b.astype(BF16), preferred_element_type=F32)


def dot_t(a, b):
    dims = (((1,), (1,)), ((), ()))
    return lax.dot_general(a.astype(BF16), b.astype(BF16), dims, preferred_element_type=F32)


def dot_of_t(a, b):
    dims = (((0,), (0,)), ((), ()))
    return lax.dot_general(a.astype(BF16), b.astype(BF16), dims, preferred_element_type=F32)


def silu(a):
    return a * jax.nn.sigmoid(a)


def unit_rows(a):
    return a * lax.rsqrt(jnp.sum(a * a, axis=-1, keepdims=True) + EPS)


def unit_lower_inverses(blocks, row, col):
    size = blocks[0].shape[0]
    eye = jnp.where(row == col, 1.0, 0.0)
    below = (row - col == 1) & (lax.rem(row, 2) == 1)
    inverses = [eye - jnp.where(below, a, 0.0) for a in blocks]
    width = 2
    while width < size:
        same = lax.div(row, 2 * width) == lax.div(col, 2 * width)
        mask = same & (lax.div(row, width) != lax.div(col, width))
        steps = [dot(b, jnp.where(mask, a, 0.0)) for a, b in zip(blocks, inverses)]
        inverses = [b - dot(p, b) for p, b in zip(steps, inverses)]
        width *= 2
    return inverses


def kernel(
    nz,
    paired,
    tok_ref,
    k_ref,
    v_ref,
    q_ref,
    up_ref,
    gate_ref,
    do_ref,
    co_ref,
    gain_ref,
    decay_ref,
    strength_ref,
    spike_ref,
    s0_ref,
    rate_ref,
    bias_ref,
    head_gain_ref,
    taps_ref,
    channel_gain_ref,
    out_ref,
    tok,
    normed,
    wbuf,
    wout,
    gates,
    spikes,
    start,
    keys_at,
    gammas,
    growth,
    solved,
    base,
    reader,
    map_out,
    map_in,
    states,
    state_in,
    rim_out,
    rim_in,
    extended,
    conv_out,
    conv_all,
    attn_out,
    attn_all,
    partial,
    ring_send,
    ring_recv,
    y_send,
    y_recv,
    near_send,
    near_recv,
    far_send,
    far_recv,
    own_send,
    own_recv,
    t_send,
    t_recv,
    c_send,
    c_recv,
    k_send,
    k_recv,
    s_send,
    s_recv,
    local,
    map_send,
    map_recv,
    state_send,
    state_recv,
    rim_sem,
    conv_send,
    conv_recv,
    attn_send,
    attn_recv,
):
    z, x, c = lax.axis_index("sp"), lax.axis_index("fs"), lax.axis_index("tp")
    up, down = turn(z + 1, nz), turn(z - 1, nz)
    right, left, over = turn(x + 1, NX), turn(x - 1, NX), turn(x + 2, NX)
    other = 1 - c
    head = c * NX + x
    half = nz // 2
    quarter = nz // NX
    last = nz - 1
    rows, features = tok_ref.shape
    seq_me, is_composer = composer(z, c, nz)
    group = lax.axis_index("grp")
    parity = lax.rem(group, 2)
    partner = group + 1 - 2 * parity

    neighbours = [{"sp": up}, {"sp": down}, {"fs": right}, {"fs": left}, {"fs": over}, {"tp": other}]
    neighbours += [{"fs": right, "tp": other}, {"fs": left, "tp": other}, {"fs": over, "tp": other}]
    if paired:
        neighbours.append({"grp": partner})
    barrier = pltpu.get_barrier_semaphore()
    for where in neighbours:
        pl.semaphore_signal(barrier, inc=1, device_id=where, device_id_type=MESH)

    own = [w.at[:, lanes(x)] for w in (k_ref, v_ref, q_ref, up_ref, gate_ref)]
    own += [w.at[lanes(x), :] for w in (do_ref, co_ref)]
    copies = [pltpu.make_async_copy(a, wbuf.at[z, j], local.at[j]) for j, a in enumerate(own)]
    copies.append(pltpu.make_async_copy(tok_ref, tok.at[x, c], local.at[7]))
    for copy in copies:
        copy.start()

    row = lax.broadcasted_iota(jnp.int32, (rows, rows), 0)
    col = lax.broadcasted_iota(jnp.int32, (rows, rows), 1)

    def to_row(column):
        return jnp.sum(jnp.where(row == col, column, 0.0), axis=0, keepdims=True)

    def to_column(line):
        return jnp.sum(jnp.where(row == col, line, 0.0), axis=1, keepdims=True)

    if paired:
        chunks, shared = [0, 1, 2, 3 + parity, 5 + parity], (3, 4)
    else:
        chunks, shared = list(range(7)), ()
    count = len(chunks)

    def hop(t, pos, way, src):
        ref = wbuf.at[src, chunks[pos]]
        return remote(ref, ref, ring_send.at[way, t, pos], ring_recv.at[way, t, pos], sp=up if way == 0 else down)

    def to_partner(src, i):
        ref = wbuf.at[src, chunks[shared[i]]]
        return remote(ref, ref, y_send.at[src, i], y_recv.at[src, i], grp=partner)

    def whole_piece(src):
        if paired:
            arrived(wbuf.at[src, 6 - parity], y_recv.at[src, 1])

    def spread(src):
        core, zz = lax.div(src, half), lax.rem(src, half)
        other_core = core + c - 2 * core * c
        piece, target = wbuf.at[src, pl.ds(5, 2)], wout.at[head, zz]
        remote(piece, target, near_send.at[0, src], near_recv.at[0, other_core, zz], fs=right, tp=core).start()
        remote(piece, target, near_send.at[1, src], near_recv.at[1, other_core, zz], fs=left, tp=core).start()

        @pl.when(other_core == 0)
        def _():
            pltpu.make_async_copy(piece, target, own_recv.at[0, zz]).start()

        @pl.when(other_core == 1)
        def _():
            remote(piece, target, own_send.at[zz], own_recv.at[1, zz], tp=other).start()

    pl.semaphore_wait(barrier, len(neighbours))
    for j in range(7):
        copies[j].wait()
    for pos in range(count):
        hop(0, pos, 0, z).start()
        hop(0, pos, 1, z).start()

    part = rows // 2
    halves = (pl.ds(0, part), pl.ds(part, part))
    for i in range(2):
        src = tok_ref.at[halves[i]]
        dst = tok.at[x, c, halves[i]]
        remote(src, dst, t_send.at[0, i], t_recv.at[0, i], fs=right).start()
        remote(src, dst, t_send.at[1, i], t_recv.at[1, i], fs=left).start()
    remote(tok_ref, tok.at[x, c], c_send.at[0], c_recv.at[0], tp=other).start()
    spike_copies = [
        remote(spike_ref, spikes.at[x], k_send.at[d - 1], k_recv.at[d - 1], fs=turn(x + d, NX)) for d in (1, 2, 3)
    ]
    for copy in spike_copies:
        copy.start()
    spike_own = pltpu.make_async_copy(spike_ref, spikes.at[x], local.at[8])
    spike_own.start()

    start_sends = [
        remote(s0_ref.at[turn(x + d, NX)], start, s_send.at[d - 1], s_recv.at[0], fs=turn(x + d, NX)) for d in (1, 2, 3)
    ]

    @pl.when(is_composer & (x == seq_me))
    def _():
        for copy in start_sends:
            copy.start()
        pltpu.make_async_copy(s0_ref.at[x], start, s_recv.at[0]).start()

    spread(z)

    step = 64

    def norm(s):
        def some(i, _):
            r = pl.ds(pl.multiple_of(i * step, step), step)
            a = tok[s, 0, r, :].astype(F32)
            b = tok[s, 1, r, :].astype(F32)
            total = jnp.sum(a * a, axis=-1, keepdims=True) + jnp.sum(b * b, axis=-1, keepdims=True)
            scale = lax.rsqrt(total * (1.0 / (2 * features)) + EPS)
            at = pl.ds(pl.multiple_of(s * rows + i * step, step), step)
            normed[at, :features] = (a * scale * gain_ref[:, :features]).astype(BF16)
            normed[at, features:] = (b * scale * gain_ref[:, features:]).astype(BF16)
            return 0

        lax.fori_loop(0, rows // step, some, 0)

    def pass_on(i, src):
        remote(tok.at[src, c], tok.at[src, c], c_send.at[i], c_recv.at[i], tp=other).start()

    def tokens_near():
        for i in range(2):
            arrived(tok.at[left, c, halves[i]], t_recv.at[0, i])
            arrived(tok.at[right, c, halves[i]], t_recv.at[1, i])
        a, b = tok.at[left, c, halves[0]], tok.at[right, c, halves[1]]
        remote(a, a, t_send.at[2, 0], t_recv.at[2, 0], fs=right).start()
        remote(b, b, t_send.at[2, 1], t_recv.at[2, 1], fs=left).start()
        pass_on(1, left)
        pass_on(2, right)

    def norm_own():
        copies[7].wait()
        arrived(tok.at[x, other], c_recv.at[0])
        norm(x)

    def norm_near(i, src):
        arrived(tok.at[src, other], c_recv.at[i])
        norm(src)

    def tokens_far():
        for i in range(2):
            arrived(tok.at[over, c, halves[i]], t_recv.at[2, i])
        pass_on(3, over)

    hooks = (
        (2, norm_own),
        (4, tokens_near),
        (5, lambda: norm_near(1, left)),
        (6, lambda: norm_near(2, right)),
        (6, tokens_far),
    )

    for t in range(1, half):
        both_ways = ((0, turn(z - t, nz)), (1, turn(z + t, nz)))
        for pos in range(count):
            for way, src in both_ways:
                arrived(wbuf.at[src, chunks[pos]], ring_recv.at[way, t - 1, pos])
                if t < half - 1 or pos % 2 == way:
                    hop(t, pos, way, src).start()
        for i in range(len(shared)):
            for way, src in both_ways:
                to_partner(src, i).start()
        if t >= 2:
            for src in (turn(z - t + 1, nz), turn(z + t - 1, nz)):
                whole_piece(src)
                spread(src)
        for when, task in hooks:
            if t == min(when, half - 1):
                task()
    norm_near(3, over)
    for src in (turn(z - half + 1, nz), turn(z + half - 1, nz)):
        whole_piece(src)
        spread(src)
    far = turn(z + half, nz)

    def last_hop(positions):
        for pos in positions:
            arrived(wbuf.at[far, chunks[pos]], ring_recv.at[pos % 2, half - 1, pos])

    last_hop(range(2))

    for d in (1, 2, 3):
        arrived(spikes.at[turn(x - d, NX)], k_recv.at[d - 1])
    spike_own.wait()

    def matrix(*js):
        return jnp.concatenate([wbuf[:, j].reshape(nz * HEAD, HEAD) for j in js], axis=1)

    def rows_of(s):
        return pl.ds(pl.multiple_of(s * rows, rows), rows)

    small = jnp.concatenate([decay_ref[...], strength_ref[...]], axis=0)
    for s in range(NX):
        gates[s] = dot_t(small, normed[s * rows : (s + 1) * rows, :])
    rate = jnp.exp(jnp.full((1, rows), rate_ref[head], F32))
    bias = bias_ref[head]
    edge = rows // 2
    row_half = lax.broadcasted_iota(jnp.int32, (edge, edge), 0)
    col_half = lax.broadcasted_iota(jnp.int32, (edge, edge), 1)

    def rounded(a):
        return a.astype(BF16).astype(F32)

    def terms(s):
        raw = rounded(jnp.dot(normed[rows_of(s), :], matrix(0, 1), preferred_element_type=F32))
        keys = unit_rows(silu(raw[:, :HEAD]))
        values = silu(raw[:, HEAD:])
        logit = rounded(gates[s, pl.ds(head, 1), :])
        beta = to_column(jax.nn.sigmoid(rounded(gates[s, pl.ds(HEADS + head, 1), :]) + bias))
        soft = jnp.maximum(logit, 0.0) + jnp.log1p(jnp.exp(-jnp.abs(logit)))
        log_row = spikes[s, pl.ds(x, 1), :] - rate * soft
        cum_col = jnp.sum(jnp.where(col <= row, log_row, 0.0), axis=1, keepdims=True)
        cum_row = to_row(cum_col)
        gamma = jnp.where(col <= row, jnp.exp(jnp.minimum(cum_col - cum_row, 0.0)), 0.0)
        grown = jnp.exp(cum_col)
        a_matrix = jnp.where(col < row, beta * dot_t(keys, keys) * gamma, 0.0)
        right = jnp.concatenate([beta * values, (beta * grown) * keys], axis=1).astype(BF16)
        total = cum_col[rows - 1 :, :]
        decayed = (keys * jnp.exp(total - cum_col)).astype(BF16)
        keys_at[s] = keys.astype(BF16)
        gammas[s] = gamma
        growth[s] = jnp.broadcast_to(grown, (rows, HEAD))
        return a_matrix, right, decayed, total

    def finish(group_of, all_terms):
        blocks = []
        for a_matrix, _, _, _ in all_terms:
            blocks += [a_matrix[:edge, :edge], a_matrix[edge:, edge:]]
        inverses = unit_lower_inverses(blocks, row_half, col_half)
        for n, s in enumerate(group_of):
            a_matrix, right, decayed, total = all_terms[n]
            first, second_half = inverses[2 * n], inverses[2 * n + 1]
            top = dot(first, right[:edge])
            low = dot(second_half, right[edge:].astype(F32) - dot(a_matrix[edge:, :edge], top))
            both = jnp.concatenate([top, low], axis=0).astype(BF16)
            solved[s] = both
            keep = jnp.exp(total)
            keep_hi = rounded(keep)
            tail = lax.broadcasted_iota(jnp.int32, (8, 2 * HEAD), 0)
            map_out[s, 0:HEAD, :] = dot_of_t(decayed, both).astype(BF16)
            map_out[s, HEAD:, :] = jnp.where(tail < 4, keep_hi, keep - keep_hi).astype(BF16)

    def send_map(s):
        owner = s * quarter + other * (quarter // 2)

        @pl.when((z != owner) & (z != last))
        def _():
            remote(map_out.at[s], map_in.at[z], map_send.at[s], map_recv.at[z], sp=owner).start()

        @pl.when((z == owner) & (z != last))
        def _():
            pltpu.make_async_copy(map_out.at[s], map_in.at[z], map_recv.at[z]).start()

    def reads(s):
        at = rows_of(s)
        raw = rounded(jnp.dot(normed[at, :], matrix(2), preferred_element_type=F32))
        query = unit_rows(silu(raw)) * HEAD ** (-0.5)
        scores = dot_t(query, keys_at[s]) * gammas[s]
        read = dot(scores, solved[s])
        base[s] = read[:, :HEAD]
        reader[s] = (growth[s] * query - read[:, HEAD:]).astype(BF16)

    here = lax.div(z, quarter)
    far_pair = [lax.rem(here + k, NX) for k in (2, 1)]
    near_pair = [lax.rem(here + k, NX) for k in (3, 0)]
    pending = [terms(s) for s in far_pair]
    last_hop(range(2, count))
    for i in range(len(shared)):
        to_partner(far, i).start()
    finish(far_pair, pending)
    pending = [terms(s) for s in near_pair]
    for s in far_pair:
        send_map(s)
    whole_piece(far)
    spread(far)
    finish(near_pair, pending)
    reads(far_pair[0])
    for s in near_pair:
        send_map(s)
    if paired:

        def shared_in(d, _):
            src = turn(z + d, nz)
            arrived(wbuf.at[src, 4 - parity], y_recv.at[src, 0])
            return 0

        lax.fori_loop(1, nz, shared_in, 0)

    def second(zz, _):
        for rel, core in ((0, c), (1, other)):
            first, again = wout.at[core * NX + left, zz], wout.at[core * NX + right, zz]
            arrived(first, near_recv.at[0, rel, zz])
            remote(first.at[0], first.at[0], far_send.at[0, rel, zz], far_recv.at[0, rel, zz], fs=right).start()
            arrived(again, near_recv.at[1, rel, zz])
            remote(again.at[1], again.at[1], far_send.at[1, rel, zz], far_recv.at[1, rel, zz], fs=left).start()
        return 0

    lax.fori_loop(0, half, second, 0)

    def gated(s):
        at = pl.ds(s * rows, rows)
        raw = rounded(jnp.dot(normed[at, :], matrix(3, 4), preferred_element_type=F32))
        glu = (raw[:, :HEAD] * jax.nn.sigmoid(raw[:, HEAD:])).astype(BF16)
        extended[s, pl.ds(PAD, rows), :] = glu.astype(F32)
        rim_out[s] = glu[rows - PAD :]

    for s in range(NX):
        gated(s)
    reads(far_pair[1])

    @pl.when(z < last)
    def _():
        remote(rim_out, rim_in, rim_sem.at[0], rim_sem.at[1], sp=z + 1).start()

    for s in near_pair:
        reads(s)

    @pl.when(z > 0)
    def _():
        arrived(rim_in, rim_sem.at[1])
        extended[:, 0:PAD, :] = rim_in[...].astype(F32)

    @pl.when(z == 0)
    def _():
        extended[:, 0:PAD, :] = jnp.zeros((NX, PAD, HEAD), F32)

    piece = 64
    taps = taps_ref[:, lanes(head)]
    for s in range(NX):
        for r in range(rows // piece):
            conv = jnp.zeros((piece, HEAD), F32)
            for tap in range(KSIZE):
                conv = conv + taps[tap : tap + 1] * extended[s, pl.ds(r * piece + tap + PAD - KSIZE + 1, piece), :]
            conv_out[s, pl.ds(r * piece, piece), :] = conv.astype(BF16)

    def give(i):
        @pl.when(i != z)
        def _():
            remote(states.at[i], state_in.at[seq_me], state_send.at[i], state_recv.at[seq_me], sp=i).start()

        @pl.when(i == z)
        def _():
            pltpu.make_async_copy(states.at[i], state_in.at[seq_me], state_recv.at[seq_me]).start()

    @pl.when(is_composer)
    def _():
        arrived(start, s_recv.at[0])
        states[0] = start[...].astype(BF16)

        def advance(i, state):
            give(i)
            arrived(map_in.at[i], map_recv.at[i])
            block = map_in[i]
            keep = block[HEAD : HEAD + 1, :HEAD].astype(F32) + block[HEAD + 4 : HEAD + 5, :HEAD].astype(F32)
            high = state.astype(BF16)
            low = state - high.astype(F32)
            reduce = dot(block[:HEAD, HEAD:], high) + dot(block[:HEAD, HEAD:], low)
            result = keep * state - reduce + block[:HEAD, :HEAD].astype(F32)
            states[i + 1] = result.astype(BF16)
            return result

        lax.fori_loop(0, last, advance, start[...])

    def exchange(src, dst, send, recv):
        for d in range(NX):
            s = turn(x + d, NX)
            if d == 0:
                pltpu.make_async_copy(src.at[s], dst.at[:, lanes(head)], recv.at[0]).start()
            else:
                remote(src.at[s], dst.at[:, lanes(head)], send.at[d], recv.at[d], fs=s).start()
            remote(src.at[s], dst.at[:, lanes(head)], send.at[NX + d], recv.at[NX + d], fs=s, tp=other).start()

    def exchanged(src, dst, send, recv):
        for d in range(NX):
            source = turn(x - d, NX)
            arrived(dst.at[:, lanes(c * NX + source)], recv.at[d])
            arrived(dst.at[:, lanes(other * NX + source)], recv.at[NX + d])
            if d:
                remote(src.at[0], dst.at[:, lanes(head)], send.at[d], recv.at[d], fs=right).wait_send()
            remote(src.at[0], dst.at[:, lanes(head)], send.at[NX + d], recv.at[NX + d], fs=right).wait_send()

    exchange(conv_out, conv_all, conv_send, conv_recv)
    pl.when(is_composer)(lambda: give(last))

    head_gain = head_gain_ref[...]
    target = attn_all.at[:, lanes(head)]

    def send_attn(s):
        d = turn(s - x, NX)

        @pl.when(d == 0)
        def _():
            pltpu.make_async_copy(attn_out.at[s], target, attn_recv.at[0]).start()

        @pl.when(d != 0)
        def _():
            remote(attn_out.at[s], target, attn_send.at[d], attn_recv.at[d], fs=s).start()

        remote(attn_out.at[s], target, attn_send.at[NX + d], attn_recv.at[NX + d], fs=s, tp=other).start()

    order = [lax.rem(here + k, NX) for k in (0, 1, 3, 2)]
    for n, s in enumerate(order):
        arrived(state_in.at[s], state_recv.at[s])
        attn = base[s] + jnp.dot(reader[s], state_in[s], preferred_element_type=F32)
        scale = lax.rsqrt(jnp.mean(attn * attn, axis=-1, keepdims=True) + EPS)
        attn_out[s] = (attn * scale * head_gain).astype(BF16)
        if n:
            send_attn(order[n - 1])
    send_attn(order[-1])
    exchanged(conv_out, conv_all, conv_send, conv_recv)

    def channel_norm(i, _):
        at = pl.ds(pl.multiple_of(i * 64, 64), 64)
        conv = conv_all[at, :].astype(F32)
        mean = jnp.mean(conv, axis=-1, keepdims=True)
        var = jnp.mean(conv * conv, axis=-1, keepdims=True) - mean * mean
        conv_all[at, :] = silu((conv - mean) * lax.rsqrt(var + EPS) * channel_gain_ref[...]).astype(BF16)
        return 0

    lax.fori_loop(0, rows // 64, channel_norm, 0)

    def weights_in(zz, _):
        arrived(wout.at[head, zz], own_recv.at[0, zz])
        arrived(wout.at[other * NX + x, zz], own_recv.at[1, zz])
        for rel, core in ((0, c), (1, other)):
            for kind in range(2):
                arrived(wout.at[core * NX + over, zz, kind], far_recv.at[kind, rel, zz])
        return 0

    lax.fori_loop(0, half, weights_in, 0)

    def weights(j, kind):
        pair = [wout[:, 2 * j + i, kind].reshape(HEADS * HEAD, HEAD) for i in range(2)]
        return jnp.concatenate(pair, axis=1)

    def conv_part(j, _):
        partial[j] = jnp.dot(conv_all[...], weights(j, 1), preferred_element_type=F32)
        return 0

    lax.fori_loop(0, half // 2, conv_part, 0)
    def drain_ring(t, _):
        for pos in range(count):
            for way in range(2):
                hop(t, pos, way, z).wait_send()
        return 0

    lax.fori_loop(0, half - 1, drain_ring, 0)
    for pos in range(count):
        hop(half - 1, pos, pos % 2, z).wait_send()
    for i in range(2):
        for where, line in ((right, 0), (left, 1), (right, 2)):
            ref = tok.at[x, c, halves[i]]
            remote(ref, ref, t_send.at[line, i], t_recv.at[line, i], fs=where).wait_send()
    for i in range(4):
        remote(tok.at[x, c], tok.at[x, c], c_send.at[i], c_recv.at[i], tp=other).wait_send()
    for copy in spike_copies:
        copy.wait_send()

    @pl.when(is_composer & (x == seq_me))
    def _():
        for copy in start_sends:
            copy.wait_send()

    def drain(i, _):
        for way in range(2):
            remote(wbuf.at[i, pl.ds(5, 2)], wout.at[head, 0], near_send.at[way, i], near_recv.at[way, 0, 0], fs=right).wait_send()
        if paired:

            @pl.when(i != z)
            def _():
                to_partner(i, 0).wait_send()
                to_partner(i, 1).wait_send()

        @pl.when(is_composer & (i != z))
        def _():
            remote(states.at[i], state_in.at[seq_me], state_send.at[i], state_recv.at[seq_me], sp=i).wait_send()

        return 0

    lax.fori_loop(0, nz, drain, 0)

    def drain_half(zz, _):
        remote(wbuf.at[0, pl.ds(5, 2)], wout.at[head, zz], own_send.at[zz], own_recv.at[1, zz], tp=other).wait_send()
        for way in range(2):
            for rel in range(2):
                ref = wout.at[head, zz, 0]
                remote(ref, ref, far_send.at[way, rel, zz], far_recv.at[way, rel, zz], fs=right).wait_send()
        return 0

    lax.fori_loop(0, half, drain_half, 0)
    for s in range(NX):

        @pl.when((z != s * quarter + other * (quarter // 2)) & (z != last))
        def _(s=s):
            remote(map_out.at[s], map_in.at[z], map_send.at[s], map_recv.at[z], sp=0).wait_send()

    @pl.when(z < last)
    def _():
        remote(rim_out, rim_in, rim_sem.at[0], rim_sem.at[1], sp=z + 1).wait_send()

    exchanged(attn_out, attn_all, attn_send, attn_recv)

    def attn_part(j, _):
        total = partial[j] + jnp.dot(attn_all[...], weights(j, 0), preferred_element_type=F32)
        out_ref[:, pl.ds(pl.multiple_of(j * 2 * HEAD, 2 * HEAD), 2 * HEAD)] = total.astype(BF16)
        return 0

    lax.fori_loop(0, half // 2, attn_part, 0)


def mixed_tokens(nz, paired, tokens, *rest):
    rows, features = tokens.shape
    half = nz // 2
    count = 5 if paired else 7
    vmem = pl.BlockSpec(memory_space=pltpu.VMEM)
    smem = pl.BlockSpec(memory_space=pltpu.SMEM)
    dma = pltpu.SemaphoreType.DMA
    width = HEADS * HEAD
    return pl.pallas_call(
        functools.partial(kernel, nz, paired),
        name="mix",
        out_shape=jax.ShapeDtypeStruct((rows, half * HEAD), BF16),
        in_specs=[vmem] * 13 + [smem] * 2 + [vmem] * 3,
        out_specs=vmem,
        scratch_shapes=[
            pltpu.VMEM((NX, 2, rows, features), BF16),
            pltpu.VMEM((NX * rows, 2 * features), BF16),
            pltpu.VMEM((nz, 7, HEAD, HEAD), BF16),
            pltpu.VMEM((HEADS, half, 2, HEAD, HEAD), BF16),
            pltpu.VMEM((NX, 2 * HEADS, rows), F32),
            pltpu.VMEM((NX, NX, rows), F32),
            pltpu.VMEM((HEAD, HEAD), F32),
            pltpu.VMEM((NX, rows, HEAD), BF16),
            pltpu.VMEM((NX, rows, rows), F32),
            pltpu.VMEM((NX, rows, HEAD), F32),
            pltpu.VMEM((NX, rows, 2 * HEAD), BF16),
            pltpu.VMEM((NX, rows, HEAD), F32),
            pltpu.VMEM((NX, rows, HEAD), BF16),
            pltpu.VMEM((NX, HEAD + 8, 2 * HEAD), BF16),
            pltpu.VMEM((nz, HEAD + 8, 2 * HEAD), BF16),
            pltpu.VMEM((nz, HEAD, HEAD), BF16),
            pltpu.VMEM((NX, HEAD, HEAD), BF16),
            pltpu.VMEM((NX, PAD, HEAD), BF16),
            pltpu.VMEM((NX, PAD, HEAD), BF16),
            pltpu.VMEM((NX, PAD + rows, HEAD), F32),
            pltpu.VMEM((NX, rows, HEAD), BF16),
            pltpu.VMEM((rows, width), BF16),
            pltpu.VMEM((NX, rows, HEAD), BF16),
            pltpu.VMEM((rows, width), BF16),
            pltpu.VMEM((half // 2, rows, 2 * HEAD), F32),
            dma((2, half, count)),
            dma((2, half, count)),
            dma((nz, 2)),
            dma((nz, 2)),
            dma((2, nz)),
            dma((2, 2, half)),
            dma((2, 2, half)),
            dma((2, 2, half)),
            dma((half,)),
            dma((2, half)),
            dma((3, 2)),
            dma((3, 2)),
            dma((4,)),
            dma((4,)),
            dma((3,)),
            dma((3,)),
            dma((3,)),
            dma((1,)),
            dma((9,)),
            dma((NX,)),
            dma((nz,)),
            dma((nz,)),
            dma((NX,)),
            dma((2,)),
            dma((2 * NX,)),
            dma((2 * NX,)),
            dma((2 * NX,)),
            dma((2 * NX,)),
        ],
        compiler_params=pltpu.CompilerParams(
            collective_id=0, has_side_effects=True, vmem_limit_bytes=60 * 1024 * 1024
        ),
    )(tokens, *rest)


def on_device(
    nz,
    paired,
    tokens,
    input_norm_gain,
    query_weight,
    key_weight,
    value_weight,
    decay_gate_weight,
    write_strength_weight,
    up_weight,
    gate_half_weight,
    log_decay_rate,
    write_strength_bias,
    decay_spike_added,
    starting_state,
    head_norm_gain,
    convolution_kernel,
    channel_norm_gain,
    delta_output_rows,
    convolution_output_rows,
):
    mixed = mixed_tokens(
        nz,
        paired,
        tokens[0],
        key_weight,
        value_weight,
        query_weight,
        up_weight,
        gate_half_weight,
        delta_output_rows,
        convolution_output_rows,
        input_norm_gain[None],
        decay_gate_weight.T,
        write_strength_weight.T,
        decay_spike_added[0].T,
        starting_state[0],
        log_decay_rate,
        write_strength_bias,
        head_norm_gain[None],
        convolution_kernel,
        channel_norm_gain[None],
    )
    return mixed[None]


def solution(mesh):
    return jax.shard_map(
        functools.partial(on_device, mesh.shape["sp"], mesh.shape["grp"] % 2 == 0),
        mesh=mesh,
        in_specs=(
            P(("grp", "fs"), "sp", "tp"),
            P(),
            P("sp", "tp"),
            P("sp", "tp"),
            P("sp", "tp"),
            P(),
            P(),
            P("sp", "tp"),
            P("sp", "tp"),
            P(),
            P(),
            P(("grp", "fs"), "sp", "tp"),
            P(("grp", "fs"), "tp", None, None),
            P(),
            P(),
            P(),
            P("tp", "sp"),
            P("tp", "sp"),
        ),
        out_specs=P(("grp", "fs"), "sp", "tp"),
        check_vma=False,
    )
```
